32 devices in a mesh: sp: 16 (over z, y, x), tp: 2 (over core).
Axes of the slice: x: 2, y: 2, z: 4, core: 2. Of those that a mesh axis runs over, the one named last changes fastest.
Arguments:
- residual: bfloat16 [2048, 2048], P('sp'), may hold values from -6 to 6
- query_first: bfloat16 [2048, 8, 128], P('sp', 'tp'), may hold values from -6.5 to 6.5
- key_first: bfloat16 [2048, 8, 128], P('sp', 'tp'), may hold values from -6.5 to 6.5
- value_first: bfloat16 [2048, 8, 128], P('sp', 'tp'), may hold values from -6 to 6
- query_second: bfloat16 [2048, 8, 64], P('sp', 'tp'), may hold values from -6.5 to 6.5
- key_second: bfloat16 [2048, 8, 64], P('sp', 'tp'), may hold values from -6.5 to 6.5
- value_second: bfloat16 [2048, 8, 64], P('sp', 'tp'), may hold values from -6 to 6
- balance_first: float32 [8], P('tp'), may hold values from 0.3 to 0.8
- balance_second: float32 [8], P('tp'), may hold values from 0.3 to 0.8
- head_gain_first: float32 [128], replicated, may hold values from 0.1 to 1.9
- head_gain_second: float32 [64], replicated, may hold values from 0.1 to 1.9
- out_first: bfloat16 [1024, 2048], P('tp'), may hold values from -0.15625 to 0.15625
- out_second: bfloat16 [512, 2048], P('tp'), may hold values from -0.15625 to 0.15625
- mlp_gain: float32 [2048], replicated, may hold values from 0.1 to 1.9
- up_weight: bfloat16 [2048, 8192], P('sp', 'tp'), may hold values from -0.125 to 0.125
- down_weight: bfloat16 [2048, 8192], P('sp', 'tp'), may hold values from -0.0625 to 0.0625
Outputs:
- layer_out: bfloat16 [2048, 2048], P('sp')
The draws below stay inside these ranges and needn't reach their ends.
All inputs are finite; a program needn't handle non-finite values.
Results may differ from the reference program's by a relative error of at most 0.018.
Values may be sent and summed in bfloat16 or wider, within the bound.
A program may use at most 128 MiB of HBM per device.

```python
import math
import jax
import jax.numpy as jnp
from jax import lax

D = 2048
FF = 8192
HEADS_A = 8
HEADS_B = 8
DK_A = 64
DV_A = 128
DK_B = 32
DV_B = 64
SEQ = 2048
N_TP = 2


def drawn(key, heads, head_size):
    width = 2 * head_size
    queries = jnp.clip(1.3 * jax.random.normal(jax.random.fold_in(key, 11), (SEQ, heads, width), jnp.float32), -6.5, 6.5)
    keys = jnp.clip(1.3 * jax.random.normal(jax.random.fold_in(key, 12), (SEQ, heads, width), jnp.float32), -6.5, 6.5)
    return (queries, keys)


def draw_query_first(key, part):
    return drawn(jax.random.fold_in(key, 1), HEADS_A, DK_A)[0].astype(jnp.bfloat16)


def draw_key_first(key, part):
    return drawn(jax.random.fold_in(key, 1), HEADS_A, DK_A)[1].astype(jnp.bfloat16)


def draw_query_second(key, part):
    return drawn(jax.random.fold_in(key, 2), HEADS_B, DK_B)[0].astype(jnp.bfloat16)


def draw_key_second(key, part):
    return drawn(jax.random.fold_in(key, 2), HEADS_B, DK_B)[1].astype(jnp.bfloat16)


def block_scale(key, dims, shards, smallest, high):
    loudness = 1.0
    for position, parts in shards:
        draws = jax.random.uniform(jax.random.fold_in(jax.random.fold_in(key, 6), position), (parts,), jnp.float32, smallest / len(shards), high / len(shards))
        loudness = loudness * jnp.repeat(jnp.exp(draws), dims[position] // parts).reshape((-1,) + (1,) * (len(dims) - 1 - position))
    return loudness


def gaussian(rng, shape, spread, limit, split=(), kind=jnp.bfloat16):
    values = spread * jax.random.normal(rng, shape, jnp.float32)
    if split:
        values = values * block_scale(rng, shape, split, -0.22, 0.18)
    return jnp.clip(values, -limit, limit).astype(kind)


def setup_inputs(seed: int = 0) -> dict:
    key_list = jax.random.split(jax.random.key(seed), 17)
    return {
        "residual": gaussian(key_list[0], (SEQ, D), 1.0, 6.0, ((0, 16),)),
        "query_first": draw_query_first(jax.random.fold_in(key_list[16], 71), 0),
        "key_first": draw_key_first(jax.random.fold_in(key_list[16], 71), 0),
        "value_first": gaussian(key_list[3], (SEQ, HEADS_A, DV_A), 1.0, 6.0, ((0, 16), (1, 2))),
        "query_second": draw_query_second(jax.random.fold_in(key_list[16], 71), 0),
        "key_second": draw_key_second(jax.random.fold_in(key_list[16], 71), 0),
        "value_second": gaussian(key_list[6], (SEQ, HEADS_B, DV_B), 1.0, 6.0, ((0, 16), (1, 2))),
        "balance_first": jnp.clip(0.3 + 0.5 * jax.random.uniform(key_list[7], (HEADS_A,), jnp.float32) ** block_scale(key_list[7], (HEADS_A,), ((0, 2),), -0.2, 0.2), 0.3, 0.8),
        "balance_second": jnp.clip(0.3 + 0.5 * jax.random.uniform(key_list[8], (HEADS_B,), jnp.float32) ** block_scale(key_list[8], (HEADS_B,), ((0, 2),), -0.2, 0.2), 0.3, 0.8),
        "head_gain_first": jnp.clip(1.0 + 0.18 * jax.random.normal(key_list[9], (DV_A,), jnp.float32), 0.1, 1.9),
        "head_gain_second": jnp.clip(1.0 + 0.18 * jax.random.normal(key_list[10], (DV_B,), jnp.float32), 0.1, 1.9),
        "out_first": gaussian(key_list[11], (HEADS_A * DV_A, D), (HEADS_A * DV_A + HEADS_B * DV_B) ** -0.5, 0.15625, ((0, 2),)),
        "out_second": gaussian(key_list[12], (HEADS_B * DV_B, D), (HEADS_A * DV_A + HEADS_B * DV_B) ** -0.5, 0.15625, ((0, 2),)),
        "mlp_gain": jnp.clip(1.0 + 0.18 * jax.random.normal(key_list[13], (D,), jnp.float32), 0.1, 1.9),
        "up_weight": gaussian(key_list[14], (D, FF), D ** -0.5, 0.125, ((0, 16), (1, 2))),
        "down_weight": gaussian(key_list[15], (D, FF), FF ** -0.5, 0.0625, ((0, 16), (1, 2))),
    }


EPSILON = 1e-06
HEAD_SCALE = 0.8

def group_heads(queries, keys, values, balance, gain, head_size):
    seq = queries.shape[0]
    heads = queries.shape[1]
    depth = values.shape[2]
    block = math.gcd(256, seq)
    count = seq // block
    query_maps = queries.astype(jnp.float32).reshape(count, block, heads, 2, head_size)
    key_maps = keys.astype(jnp.float32).reshape(seq, heads, 2, head_size)
    value_float = values.astype(jnp.float32)
    columns = jnp.arange(seq, dtype=jnp.int32)
    gain_float = gain.astype(jnp.float32)

    def one_block(args):
        query_block, start = args
        scores = jnp.einsum('qhmd,khmd->hmqk', query_block, key_maps) * head_size ** (-0.5)
        positions = start + jnp.arange(block, dtype=jnp.int32)
        scores = jnp.where(columns[None, :] <= positions[:, None], scores, -jnp.inf)
        probs = jax.nn.softmax(scores, axis=-1)
        mixed = (probs[:, 0] - balance[:, None, None] * probs[:, 1]).astype(jnp.bfloat16)
        mixed = lax.optimization_barrier(mixed).astype(jnp.float32)
        summed = jnp.einsum('hqk,khe->qhe', mixed, value_float)
        power = lax.optimization_barrier(jnp.mean(summed * summed, axis=-1, keepdims=True))
        normed = summed * lax.rsqrt(power + EPSILON) * gain_float * HEAD_SCALE
        return normed.astype(jnp.bfloat16)
    starts = jnp.arange(count, dtype=jnp.int32) * block
    result = lax.map(one_block, (query_maps, starts))
    return result.reshape(seq, heads * depth)

def reference(residual, query_first, key_first, value_first, query_second, key_second, value_second, balance_first, balance_second, head_gain_first, head_gain_second, out_first, out_second, mlp_gain, up_weight, down_weight):
    heads_first = group_heads(query_first, key_first, value_first, balance_first, head_gain_first, DK_A)
    heads_second = group_heads(query_second, key_second, value_second, balance_second, head_gain_second, DK_B)
    seq = residual.shape[0]
    width = residual.shape[1]
    width_first = heads_first.shape[1] // N_TP
    width_second = heads_second.shape[1] // N_TP

    def head_part(number, total):
        offset_first = (number * width_first).astype(jnp.int32)
        offset_second = (number * width_second).astype(jnp.int32)
        part = jnp.dot(lax.dynamic_slice_in_dim(heads_first, offset_first, width_first, 1), lax.dynamic_slice_in_dim(out_first, offset_first, width_first, 0), preferred_element_type=jnp.float32)
        part = part + jnp.dot(lax.dynamic_slice_in_dim(heads_second, offset_second, width_second, 1), lax.dynamic_slice_in_dim(out_second, offset_second, width_second, 0), preferred_element_type=jnp.float32)
        rounded = lax.optimization_barrier(part.astype(jnp.bfloat16))
        return total + rounded.astype(jnp.float32)
    head_total = lax.fori_loop(0, N_TP, head_part, jnp.zeros((seq, width), jnp.float32))
    mixed = (residual.astype(jnp.float32) + head_total).astype(jnp.bfloat16)
    mixed_float = mixed.astype(jnp.float32)
    power = lax.optimization_barrier(jnp.mean(mixed_float * mixed_float, axis=-1, keepdims=True))
    normed = (mixed_float * lax.rsqrt(power + EPSILON) * mlp_gain.astype(jnp.float32)).astype(jnp.bfloat16)
    lifted = jnp.dot(normed, up_weight, preferred_element_type=jnp.float32)
    active = jax.nn.relu(lifted)
    hidden = (active * active).astype(jnp.bfloat16)
    width_hidden = hidden.shape[1] // N_TP

    def down_part(number, total):
        offset = (number * width_hidden).astype(jnp.int32)
        part = lax.dot_general(lax.dynamic_slice_in_dim(hidden, offset, width_hidden, 1), lax.dynamic_slice_in_dim(down_weight, offset, width_hidden, 1), (((1,), (1,)), ((), ())), preferred_element_type=jnp.float32)
        rounded = lax.optimization_barrier(part.astype(jnp.bfloat16))
        return total + rounded.astype(jnp.float32)
    down_total = lax.fori_loop(0, N_TP, down_part, jnp.zeros((seq, width), jnp.float32))
    return (mixed_float + down_total).astype(jnp.bfloat16)
```

```python
import functools
import math

import jax
import jax.numpy as jnp
from jax import lax
from jax.experimental import pallas as pl
from jax.experimental.pallas import tpu as pltpu
from jax.sharding import PartitionSpec as P

DK_A = 64
DK_B = 32


EPSILON = 1e-06
HEAD_SCALE = 0.8


def attend(queries, keys, values, balance, gain, device, head_size):
    tokens = queries.shape[0]
    heads = queries.shape[1]
    seq = keys.shape[0]
    depth = values.shape[2]
    block = math.gcd(512, seq)
    scale = head_size ** (-0.5)
    query_maps = queries.reshape(tokens, heads, 2, head_size)
    key_maps = keys.reshape(seq, heads, 2, head_size)
    first_row = device * tokens
    positions = first_row + jnp.arange(tokens, dtype=jnp.int32)
    needed = (first_row + tokens + block - 1) // block

    def block_scores(number):
        start = number * block
        key_block = lax.dynamic_slice_in_dim(key_maps, start, block, 0)
        scores = (
            jnp.einsum("qhmd,khmd->hmqk", query_maps, key_block, preferred_element_type=jnp.float32)
            * scale
        )
        columns = start + jnp.arange(block, dtype=jnp.int32)
        visible = columns[None, :] <= positions[:, None]
        return (jnp.where(visible, scores, -jnp.inf), start)

    def statistics(number, carry):
        highest, total = carry
        scores, start = block_scores(number)
        fresh = jnp.maximum(highest, jnp.max(scores, axis=-1, keepdims=True))
        total = total * jnp.exp(highest - fresh) + jnp.sum(
            jnp.exp(scores - fresh), axis=-1, keepdims=True
        )
        return (fresh, total)

    start_high = jnp.full((heads, 2, tokens, 1), -jnp.inf, jnp.float32)
    start_total = jnp.zeros((heads, 2, tokens, 1), jnp.float32)
    highest, total = lax.fori_loop(0, needed, statistics, (start_high, start_total))

    def accumulate(number, result):
        scores, start = block_scores(number)
        probs = jnp.exp(scores - highest) / total
        mixed = (probs[:, 0] - balance[:, None, None] * probs[:, 1]).astype(jnp.bfloat16)
        value_block = lax.dynamic_slice_in_dim(values, start, block, 0)
        return result + jnp.einsum(
            "hqk,khe->qhe", mixed, value_block, preferred_element_type=jnp.float32
        )

    summed = lax.fori_loop(0, needed, accumulate, jnp.zeros((tokens, heads, depth), jnp.float32))
    power = jnp.mean(summed * summed, axis=-1, keepdims=True)
    normed = summed * lax.rsqrt(power + EPSILON) * gain * HEAD_SCALE
    return normed.astype(jnp.bfloat16).reshape(tokens, heads * depth)


def body(
    residual,
    query_first,
    key_first,
    value_first,
    query_second,
    key_second,
    value_second,
    balance_first,
    balance_second,
    head_gain_first,
    head_gain_second,
    out_first,
    out_second,
    mlp_gain,
    up_weight,
    down_weight,
):
    device = lax.axis_index("sp")
    keys_first, values_first, keys_second, values_second = (
        lax.all_gather(key_first, "sp", axis=0, tiled=True),
        lax.all_gather(value_first, "sp", axis=0, tiled=True),
        lax.all_gather(key_second, "sp", axis=0, tiled=True),
        lax.all_gather(value_second, "sp", axis=0, tiled=True),
    )
    heads_first = attend(
        query_first, keys_first, values_first, balance_first, head_gain_first, device, DK_A
    )
    heads_second = attend(
        query_second, keys_second, values_second, balance_second, head_gain_second, device, DK_B
    )
    head_term = jnp.dot(heads_first, out_first, preferred_element_type=jnp.float32) + jnp.dot(
        heads_second, out_second, preferred_element_type=jnp.float32
    )
    head_total = lax.psum(head_term.astype(jnp.bfloat16), "tp").astype(jnp.float32)
    mixed = (residual.astype(jnp.float32) + head_total).astype(jnp.bfloat16)
    mixed_float = mixed.astype(jnp.float32)
    power = jnp.mean(mixed_float * mixed_float, axis=-1, keepdims=True)
    normed = (mixed_float * lax.rsqrt(power + EPSILON) * mlp_gain).astype(jnp.bfloat16)
    up_whole, down_whole = (
        lax.all_gather(up_weight, "sp", axis=0, tiled=True),
        lax.all_gather(down_weight, "sp", axis=0, tiled=True),
    )
    lifted = jnp.dot(normed, up_whole, preferred_element_type=jnp.float32)
    active = jax.nn.relu(lifted)
    hidden = (active * active).astype(jnp.bfloat16)
    down_term = lax.dot_general(
        hidden, down_whole, (((1,), (1,)), ((), ())), preferred_element_type=jnp.float32
    )
    added = lax.psum(down_term.astype(jnp.bfloat16), "tp").astype(jnp.float32)
    return (mixed_float + added).astype(jnp.bfloat16)


PLANE = 4
MESH = pl.DeviceIdType.MESH


def remote(src, dst, send_sem, recv_sem, device):
    return pltpu.make_async_remote_copy(
        src_ref=src, dst_ref=dst, send_sem=send_sem, recv_sem=recv_sem,
        device_id=device, device_id_type=MESH,
    )


def last(a, b):
    return lax.dot_general(a, b, (((1,), (1,)), ((), ())), preferred_element_type=jnp.float32)


def add(a, b):
    return (a.astype(jnp.float32) + b.astype(jnp.float32)).astype(jnp.bfloat16)


def layer_kernel(
    line, size_a, size_b,
    bal_a, bal_b, resid_h, q1_h, k1_h, v1_h, q2_h, k2_h, v2_h, gain_a, gain_b, o1_h, o2_h,
    mlp_gain, up_h, down_h,
    out,
    resid, q1, k1, v1, q2, k2, v2, o1, o2, kv_own, q_own, kv_all, q_all, heads_out, heads_in,
    up_all, down_all, part, other_part, mixed, rows, hidden, terms, held, acc, below, above, total,
    fetch, kzs, kzr, qzs, qzr, kps, kpr, uzs, uzr, ups, upr, dzs, dzr, dps, dpr, hzs, hzr,
    sws, swr, rus, rds, rr, rcs, rcr, ts, tr, cus, cds, cbr, car, fs, fr,
):
    s = lax.axis_index("sp")
    c = lax.axis_index("tp")
    z = s // PLANE
    p = s % PLANE
    x = p % 2
    y = p // 2
    flip_x = y * 2 + 1 - x
    flip_y = (1 - y) * 2 + x
    near = (1 - c) * flip_x + c * flip_y
    side = (1 - c) * flip_y + c * flip_x
    far = (1 - y) * 2 + 1 - x
    to_near = (z * PLANE + near, c)
    to_side = (z * PLANE + side, c)
    to_core = (s, 1 - c)
    to_up = (s + PLANE, c)
    to_down = (s - PLANE, c)

    tokens = kv_own.shape[1]
    wide = gain_a.shape[1]
    deep = gain_b.shape[1]
    features = resid.shape[1]
    span = PLANE * tokens
    depth = up_h.shape[0]
    width = up_all.shape[1]
    half = tokens // 2
    piece = PLANE * depth

    def fetched(number, src, dst):
        return pltpu.make_async_copy(src, dst, fetch.at[number])

    def at_place(ref, number, size):
        return ref.at[pl.ds(pl.multiple_of(number * size, size), size)]

    def columns(ref, number):
        return ref.at[:, pl.ds(pl.multiple_of(number * width, width), width)]

    small = [
        fetched(0, k1_h, k1), fetched(1, v1_h, v1), fetched(2, k2_h, k2), fetched(3, v2_h, v2),
        fetched(4, q1_h, q1), fetched(5, q2_h, q2),
    ]
    own_up = fetched(6, columns(up_h, z), at_place(up_all, s, depth))
    own_down = fetched(7, columns(down_h, z), at_place(down_all, s, depth))
    large = [fetched(8, resid_h, resid), fetched(9, o1_h, o1), fetched(10, o2_h, o2)]
    for copy in small + [own_up, own_down] + large:
        copy.start()

    barrier = pltpu.get_barrier_semaphore()
    peers = [to_near, to_side, to_core] + [(((z + j) % line) * PLANE + p, c) for j in range(1, line)]
    for device in peers:
        pl.semaphore_signal(barrier, inc=1, device_id=device, device_id_type=MESH)

    sends = []

    def send(*args):
        copy = remote(*args)
        copy.start()
        sends.append((None, copy))

    def send_if(condition, *args):
        copy = remote(*args)

        @pl.when(condition)
        def _():
            copy.start()

        sends.append((condition, copy))

    def arrived(block, sem):
        remote(block, block, fs.at[0], sem, to_core).wait_recv()

    for copy in small:
        copy.wait()
    count = tokens * line
    order = lax.broadcasted_iota(jnp.int32, (count, count), 0)
    place = lax.broadcasted_iota(jnp.int32, (count, count), 1)
    pick = jnp.where(place == (order % tokens) * line + order // tokens, 1.0, 0.0).astype(jnp.bfloat16)

    def by_head(value):
        moved = jnp.dot(pick, value, preferred_element_type=jnp.float32).astype(jnp.bfloat16)
        return moved.reshape(line, tokens, value.shape[1])

    kv_own[:, :, 0:wide] = by_head(k1[...])
    kv_own[:, :, wide:2 * wide] = by_head(v1[...])
    kv_own[:, :, 2 * wide:3 * wide] = by_head(jnp.concatenate([k2[...], v2[...]], axis=1))
    q_own[:, :, 0:wide] = by_head(q1[...])
    q_own[:, :, wide:] = by_head(q2[...])
    pl.semaphore_wait(barrier, len(peers))

    def ahead(j):
        return (z + j) % line

    def behind(j):
        return (z + line - j) % line

    def z_peer(j):
        return (ahead(j) * PLANE + p, c)

    mine = at_place(kv_all, s, tokens)
    for j in range(1, line):
        send(kv_own.at[ahead(j)], mine, kzs.at[j], kzr.at[j], z_peer(j))
    send(kv_own.at[z], mine, kps.at[0, 0], kpr.at[0, 0], to_near)
    send(kv_own.at[z], mine, kps.at[0, 1], kpr.at[0, 1], to_side)
    for j in range(1, line):
        send(q_own.at[ahead(j)], q_all.at[z], qzs.at[j], qzr.at[j], z_peer(j))
    mine[...] = kv_own[z]
    q_all[z] = q_own[z]

    weights = {
        "up": (up_h, up_all, own_up, uzs, uzr, ups, upr),
        "down": (down_h, down_all, own_down, dzs, dzr, dps, dpr),
    }

    def along(name, j):
        source, whole, _, ss, sr, _, _ = weights[name]
        send(columns(source, ahead(j)), at_place(whole, s, depth), ss.at[j], sr.at[j], z_peer(j))

    def spread(name, j):
        _, whole, own, _, sr, ss, rr_ = weights[name]
        block = at_place(whole, behind(j) * PLANE + p, depth)
        if j:
            arrived(block, sr.at[j])
        else:
            own.wait()
        send(block, block, ss.at[j, 0], rr_.at[j, 0], to_near)
        send(block, block, ss.at[j, 1], rr_.at[j, 1], to_side)

    def relay(name, j):
        _, whole, _, _, _, ss, rr_ = weights[name]
        block = at_place(whole, behind(j) * PLANE + near, depth)
        arrived(block, rr_.at[j, 0])
        send(block, block, ss.at[j, 2], rr_.at[j, 2], to_side)

    def settle(name, j):
        _, whole, _, _, _, _, rr_ = weights[name]
        for way, where in ((1, side), (2, far)):
            arrived(at_place(whole, behind(j) * PLANE + where, depth), rr_.at[j, way])

    def kv_spread(j):
        block = at_place(kv_all, behind(j) * PLANE + p, tokens)
        arrived(block, kzr.at[j])
        send(block, block, kps.at[j, 0], kpr.at[j, 0], to_near)
        send(block, block, kps.at[j, 1], kpr.at[j, 1], to_side)

    def kv_relay(j):
        block = at_place(kv_all, behind(j) * PLANE + near, tokens)
        arrived(block, kpr.at[j, 0])
        send(block, block, kps.at[j, 2], kpr.at[j, 2], to_side)

    for j in range(1, line):
        along("up", j)
    kv_spread(1)
    kv_relay(0)
    kv_spread(2)
    kv_relay(1)
    kv_spread(3)
    kv_relay(2)
    kv_relay(3)
    spread("up", 0)
    for j in range(line):
        for way, where in ((1, side), (2, far)):
            arrived(at_place(kv_all, behind(j) * PLANE + where, tokens), kpr.at[j, way])
    for j in range(1, line):
        arrived(q_all.at[behind(j)], qzr.at[j])

    lanes_a = lax.broadcasted_iota(jnp.int32, (tokens, wide), 1)
    lanes_b = lax.broadcasted_iota(jnp.int32, (tokens, deep), 1)
    line_rows = lax.broadcasted_iota(jnp.int32, (tokens, span), 0) + p * tokens
    visible = lax.broadcasted_iota(jnp.int32, (tokens, span), 1) <= line_rows

    def mix(queries, lanes, keys_at, values_at, size, b, keys_number):
        maps = []
        for m in range(2):
            chosen = (lanes >= m * size) & (lanes < (m + 1) * size)
            picked = jnp.where(chosen, queries, jnp.zeros_like(queries))
            scores = last(picked, kv_all[0:keys_number, keys_at]) * size ** (-0.5)
            tail_scores = jnp.where(visible, scores[:, keys_number - span:], -jnp.inf)
            if keys_number > span:
                scores = jnp.concatenate([scores[:, : keys_number - span], tail_scores], axis=1)
            else:
                scores = tail_scores
            powers = jnp.exp(scores - jnp.max(scores, axis=-1, keepdims=True))
            maps.append((powers, jnp.sum(powers, axis=-1, keepdims=True)))
        (e1, l1), (e2, l2) = maps
        mixing = (e1 * (1.0 / l1) - e2 * (b / l2)).astype(jnp.bfloat16)
        return jnp.dot(mixing, kv_all[0:keys_number, values_at], preferred_element_type=jnp.float32)

    def norm(value, gain):
        power = jnp.mean(value * value, axis=-1, keepdims=True)
        return (value * lax.rsqrt(power + EPSILON) * gain[...] * HEAD_SCALE).astype(jnp.bfloat16)

    def tile(j):
        number = (j + 1) * span
        first = mix(
            q_all[j, :, 0:wide], lanes_a, slice(0, wide), slice(wide, 2 * wide), size_a, bal_a[z], number
        )
        heads_out[j, :, 0:wide] = norm(first, gain_a)
        second = mix(
            q_all[j, :, wide:], lanes_b, slice(2 * wide, 2 * wide + deep),
            slice(2 * wide, 3 * wide), size_b, bal_b[z], number,
        )
        heads_out[j, :, wide:] = norm(second[:, wide - deep:wide], gain_b)
        send_if(j != z, heads_out.at[j], heads_in.at[z], hzs.at[j], hzr.at[z], (j * PLANE + p, c))

    tile(3)
    relay("up", 0)
    tile(2)
    spread("up", 1)
    tile(1)
    tile(0)
    heads_in[z] = heads_out[z]
    along("down", 1)
    along("down", 2)
    relay("up", 1)
    spread("up", 2)
    relay("up", 2)
    spread("up", 3)
    spread("down", 0)
    for copy in large:
        copy.wait()
    for h in range(line):
        block = heads_in.at[h]

        @pl.when(h != z)
        def _():
            arrived(block, hzr.at[h])

    heads_first = jnp.concatenate([heads_in[h, :, 0:wide] for h in range(line)], axis=1)
    heads_second = jnp.concatenate([heads_in[h, :, wide:] for h in range(line)], axis=1)
    step = features // 4
    for n in range(4):
        at = slice(n * step, (n + 1) * step)
        value = jnp.dot(heads_first, o1[:, at], preferred_element_type=jnp.float32) + jnp.dot(
            heads_second, o2[:, at], preferred_element_type=jnp.float32
        )
        part[:, :, at] = value.astype(jnp.bfloat16).reshape(2, half, step)
    swap = remote(part.at[1 - c], other_part, sws.at[0], swr.at[0], to_core)
    swap.start()
    relay("up", 3)
    swap.wait()
    both = part[c].astype(jnp.float32) + other_part[...].astype(jnp.float32)
    mine_rows = pl.ds(pl.multiple_of(c * half, half), half)
    mixed[...] = (resid[mine_rows, :].astype(jnp.float32) + both).astype(jnp.bfloat16)
    whole = mixed[...].astype(jnp.float32)
    power = jnp.mean(whole * whole, axis=-1, keepdims=True)
    own_slot = at_place(rows, z * 2 + c, half)
    own_slot[...] = (whole * lax.rsqrt(power + EPSILON) * mlp_gain[...]).astype(jnp.bfloat16)

    send_if(z < line - 1, own_slot, own_slot, rus.at[0], rr.at[z], to_up)
    send_if(z > 0, own_slot, own_slot, rds.at[0], rr.at[z], to_down)
    send(own_slot, own_slot, rcs.at[0], rcr.at[z], to_core)
    relay("down", 0)
    for d in range(1, line):
        from_low = at_place(rows, jnp.maximum(z - d, 0) * 2 + c, half)
        low = jnp.maximum(z - d, 0)

        @pl.when(z >= d)
        def _():
            arrived(from_low, rr.at[low])

        send_if((z >= d) & (z < line - 1), from_low, from_low, rus.at[d], rr.at[low], to_up)
        send_if(z >= d, from_low, from_low, rcs.at[d], rcr.at[low], to_core)
        high = jnp.minimum(z + d, line - 1)
        from_high = at_place(rows, high * 2 + c, half)

        @pl.when(z + d < line)
        def _():
            arrived(from_high, rr.at[high])

        send_if((z + d < line) & (z > 0), from_high, from_high, rds.at[d], rr.at[high], to_down)
        send_if(z + d < line, from_high, from_high, rcs.at[line - 1 + d], rcr.at[high], to_core)
        if d == 1:
            along("down", 3)
            spread("down", 1)
        if d == 2:
            relay("down", 1)
            spread("down", 2)
    for k in range(line):
        arrived(at_place(rows, k * 2 + 1 - c, half), rcr.at[k])
    for j in range(line):
        settle("up", j)
    relay("down", 2)

    lift = 256

    @pl.loop(0, width // lift)
    def _(n):
        at = pl.ds(pl.multiple_of(n * lift, lift), lift)
        lifted = jnp.maximum(jnp.dot(rows[...], up_all[:, at], preferred_element_type=jnp.float32), 0.0)
        hidden[:, at] = (lifted * lifted).astype(jnp.bfloat16)

    spread("down", 3)
    relay("down", 3)
    for j in range(line):
        settle("down", j)

    def chunk(k):
        at = slice(k * piece, (k + 1) * piece)
        value = last(hidden[...], down_all[k * piece:(k + 1) * piece, :]).astype(jnp.bfloat16)
        terms[:, :, :, at] = value.reshape(line, 2, half, piece)
        send(terms.at[:, 1 - c, :, at], held.at[:, :, at], ts.at[k], tr.at[k], to_core)

    def reduce(k):
        at = slice(k * piece, (k + 1) * piece)
        arrived(held.at[:, :, at], tr.at[k])
        for zd in range(line):
            acc[zd, :, at] = add(terms[zd, c, :, at], held[zd, :, at])
        for d in range(line - 1, 0, -1):
            high = jnp.minimum(z + d, line - 1)
            block = below.at[high, :, at]

            @pl.when((z + d < line) & (z > 0))
            def _():
                arrived(block, cbr.at[high, k])
                acc[high, :, at] = add(acc[high, :, at], below[high, :, at])

            send_if(z + d < line, acc.at[high, :, at], block, cus.at[d, k], cbr.at[high, k], to_up)
            low = jnp.maximum(z - d, 0)
            block = above.at[low, :, at]

            @pl.when((z >= d) & (z < line - 1))
            def _():
                arrived(block, car.at[low, k])
                acc[low, :, at] = add(acc[low, :, at], above[low, :, at])

            send_if(z >= d, acc.at[low, :, at], block, cds.at[d, k], car.at[low, k], to_down)

    def finish(k):
        at = slice(k * piece, (k + 1) * piece)
        total[...] = mixed[:, at].astype(jnp.float32) + acc[z, :, at].astype(jnp.float32)

        @pl.when(z > 0)
        def _():
            arrived(below.at[z, :, at], cbr.at[z, k])
            total[...] += below[z, :, at].astype(jnp.float32)

        @pl.when(z < line - 1)
        def _():
            arrived(above.at[z, :, at], car.at[z, k])
            total[...] += above[z, :, at].astype(jnp.float32)

        out[c, :, at] = total[...].astype(jnp.bfloat16)
        send(out.at[c, :, at], out.at[c, :, at], fs.at[k], fr.at[k], to_core)

    for k in range(line):
        chunk(k)
        if k:
            reduce(k - 1)
    reduce(line - 1)
    for k in range(line):
        finish(k)
    for k in range(line):
        at = slice(k * piece, (k + 1) * piece)
        arrived(out.at[1 - c, :, at], fr.at[k])
    for condition, copy in sends:
        if condition is None:
            copy.wait_send()
        else:

            @pl.when(condition)
            def _():
                copy.wait_send()


def layer(
    line, residual, q1, k1, v1, q2, k2, v2, bal_a, bal_b, gain_a, gain_b, o1, o2, mlp_gain, up, down
):
    tokens, features = residual.shape
    half = tokens // 2
    wide = v1.shape[1]
    deep = v2.shape[1]
    n = line * PLANE
    width = up.shape[1] // line
    depth = up.shape[0]
    b16 = jnp.bfloat16
    dma = pltpu.SemaphoreType.DMA
    vmem = pl.BlockSpec(memory_space=pltpu.VMEM)
    smem = pl.BlockSpec(memory_space=pltpu.SMEM)
    any_ = pl.BlockSpec(memory_space=pl.ANY)

    def buffer(*shape):
        return pltpu.VMEM(shape, b16)

    return pl.pallas_call(
        functools.partial(layer_kernel, line, q1.shape[1] // 2, q2.shape[1] // 2),
        out_shape=jax.ShapeDtypeStruct((2, half, features), b16),
        in_specs=[smem, smem] + [any_] * 7 + [vmem, vmem, any_, any_, vmem, any_, any_],
        out_specs=vmem,
        scratch_shapes=[
            buffer(tokens, features), buffer(*q1.shape), buffer(*k1.shape), buffer(*v1.shape),
            buffer(*q2.shape), buffer(*k2.shape), buffer(*v2.shape), buffer(*o1.shape), buffer(*o2.shape),
            buffer(line, tokens, 3 * wide), buffer(line, tokens, wide + deep),
            buffer(n * tokens, 3 * wide), buffer(line, tokens, wide + deep),
            buffer(line, tokens, wide + deep), buffer(line, tokens, wide + deep),
            buffer(n * depth, width), buffer(n * depth, width),
            buffer(2, half, features), buffer(half, features), buffer(half, features),
            buffer(line * tokens, features), buffer(line * tokens, width),
            buffer(line, 2, half, features), buffer(line, half, features), buffer(line, half, features),
            buffer(line, half, features), buffer(line, half, features),
            pltpu.VMEM((half, PLANE * depth), jnp.float32),
            dma((11,)),
            dma((line,)), dma((line,)), dma((line,)), dma((line,)), dma((line, 3)), dma((line, 3)),
            dma((line,)), dma((line,)), dma((line, 3)), dma((line, 3)),
            dma((line,)), dma((line,)), dma((line, 3)), dma((line, 3)),
            dma((line,)), dma((line,)), dma((1,)), dma((1,)),
            dma((line,)), dma((line,)), dma((line,)), dma((2 * line - 1,)), dma((line,)),
            dma((line,)), dma((line,)), dma((line, line)), dma((line, line)),
            dma((line, line)), dma((line, line)), dma((line,)), dma((line,)),
        ],
        compiler_params=pltpu.CompilerParams(
            collective_id=0, has_side_effects=True, vmem_limit_bytes=60 * 1024 * 1024
        ),
    )(bal_a, bal_b, residual, q1, k1, v1, q2, k2, v2, gain_a, gain_b, o1, o2, mlp_gain, up, down)


def placed_body(
    residual, query_first, key_first, value_first, query_second, key_second, value_second,
    balance_first, balance_second, head_gain_first, head_gain_second, out_first, out_second,
    mlp_gain, up_weight, down_weight,
):
    tokens, line, _ = query_first.shape

    def flat(array):
        return array.reshape(tokens * line, array.shape[2])

    out = layer(
        line, residual, flat(query_first), flat(key_first), flat(value_first), flat(query_second),
        flat(key_second), flat(value_second), balance_first, balance_second,
        head_gain_first[None, :], head_gain_second[None, :], out_first, out_second,
        mlp_gain[None, :], up_weight, down_weight,
    )
    return out.reshape(residual.shape)


def placed(mesh):
    ranks = mesh.shape["sp"]
    cores = mesh.shape["tp"]
    return cores == 2 and ranks % PLANE == 0


def choose(mesh):
    ranks = mesh.shape["sp"]

    def run(*arrays):
        query_first, query_second, value_second, value_first = arrays[1], arrays[4], arrays[6], arrays[3]
        fits = (
            placed(mesh)
            and query_first.shape[1] * PLANE == ranks
            and query_second.shape[1] == query_first.shape[1]
            and value_first.shape[2] == query_first.shape[2] == 128
            and query_second.shape[2] + value_second.shape[2] == query_first.shape[2]
            and query_first.shape[0] % 32 == 0
            and arrays[14].shape[1] % (128 * ranks) == 0
        )
        return (placed_body if fits else body)(*arrays)

    return run


def solution(mesh):
    in_specs = (
        P("sp", None),
        P("sp", "tp", None),
        P("sp", "tp", None),
        P("sp", "tp", None),
        P("sp", "tp", None),
        P("sp", "tp", None),
        P("sp", "tp", None),
        P("tp"),
        P("tp"),
        P(),
        P(),
        P("tp", None),
        P("tp", None),
        P(),
        P("sp", "tp"),
        P("sp", "tp"),
    )
    out_specs = P("sp", None)
    return jax.shard_map(choose(mesh), mesh=mesh, in_specs=in_specs, out_specs=out_specs, check_vma=False)
```

```python
import functools
import math

import jax
import jax.numpy as jnp
from jax import lax
from jax.experimental import pallas as pl
from jax.experimental.pallas import tpu as pltpu
from jax.sharding import PartitionSpec as P

DK_A = 64
DK_B = 32


EPSILON = 1e-06
HEAD_SCALE = 0.8


def attend(queries, keys, values, balance, gain, device, head_size):
    tokens = queries.shape[0]
    heads = queries.shape[1]
    seq = keys.shape[0]
    depth = values.shape[2]
    block = math.gcd(512, seq)
    scale = head_size ** (-0.5)
    query_maps = queries.reshape(tokens, heads, 2, head_size)
    key_maps = keys.reshape(seq, heads, 2, head_size)
    first_row = device * tokens
    positions = first_row + jnp.arange(tokens, dtype=jnp.int32)
    needed = (first_row + tokens + block - 1) // block

    def block_scores(number):
        start = number * block
        key_block = lax.dynamic_slice_in_dim(key_maps, start, block, 0)
        scores = (
            jnp.einsum("qhmd,khmd->hmqk", query_maps, key_block, preferred_element_type=jnp.float32)
            * scale
        )
        columns = start + jnp.arange(block, dtype=jnp.int32)
        visible = columns[None, :] <= positions[:, None]
        return (jnp.where(visible, scores, -jnp.inf), start)

    def statistics(number, carry):
        highest, total = carry
        scores, start = block_scores(number)
        fresh = jnp.maximum(highest, jnp.max(scores, axis=-1, keepdims=True))
        total = total * jnp.exp(highest - fresh) + jnp.sum(
            jnp.exp(scores - fresh), axis=-1, keepdims=True
        )
        return (fresh, total)

    start_high = jnp.full((heads, 2, tokens, 1), -jnp.inf, jnp.float32)
    start_total = jnp.zeros((heads, 2, tokens, 1), jnp.float32)
    highest, total = lax.fori_loop(0, needed, statistics, (start_high, start_total))

    def accumulate(number, result):
        scores, start = block_scores(number)
        probs = jnp.exp(scores - highest) / total
        mixed = (probs[:, 0] - balance[:, None, None] * probs[:, 1]).astype(jnp.bfloat16)
        value_block = lax.dynamic_slice_in_dim(values, start, block, 0)
        return result + jnp.einsum(
            "hqk,khe->qhe", mixed, value_block, preferred_element_type=jnp.float32
        )

    summed = lax.fori_loop(0, needed, accumulate, jnp.zeros((tokens, heads, depth), jnp.float32))
    power = jnp.mean(summed * summed, axis=-1, keepdims=True)
    normed = summed * lax.rsqrt(power + EPSILON) * gain * HEAD_SCALE
    return normed.astype(jnp.bfloat16).reshape(tokens, heads * depth)


def body(
    residual,
    query_first,
    key_first,
    value_first,
    query_second,
    key_second,
    value_second,
    balance_first,
    balance_second,
    head_gain_first,
    head_gain_second,
    out_first,
    out_second,
    mlp_gain,
    up_weight,
    down_weight,
):
    device = lax.axis_index("sp")
    keys_first, values_first, keys_second, values_second = (
        lax.all_gather(key_first, "sp", axis=0, tiled=True),
        lax.all_gather(value_first, "sp", axis=0, tiled=True),
        lax.all_gather(key_second, "sp", axis=0, tiled=True),
        lax.all_gather(value_second, "sp", axis=0, tiled=True),
    )
    heads_first = attend(
        query_first, keys_first, values_first, balance_first, head_gain_first, device, DK_A
    )
    heads_second = attend(
        query_second, keys_second, values_second, balance_second, head_gain_second, device, DK_B
    )
    head_term = jnp.dot(heads_first, out_first, preferred_element_type=jnp.float32) + jnp.dot(
        heads_second, out_second, preferred_element_type=jnp.float32
    )
    head_total = lax.psum(head_term.astype(jnp.bfloat16), "tp").astype(jnp.float32)
    mixed = (residual.astype(jnp.float32) + head_total).astype(jnp.bfloat16)
    mixed_float = mixed.astype(jnp.float32)
    power = jnp.mean(mixed_float * mixed_float, axis=-1, keepdims=True)
    normed = (mixed_float * lax.rsqrt(power + EPSILON) * mlp_gain).astype(jnp.bfloat16)
    up_whole, down_whole = (
        lax.all_gather(up_weight, "sp", axis=0, tiled=True),
        lax.all_gather(down_weight, "sp", axis=0, tiled=True),
    )
    lifted = jnp.dot(normed, up_whole, preferred_element_type=jnp.float32)
    active = jax.nn.relu(lifted)
    hidden = (active * active).astype(jnp.bfloat16)
    down_term = lax.dot_general(
        hidden, down_whole, (((1,), (1,)), ((), ())), preferred_element_type=jnp.float32
    )
    added = lax.psum(down_term.astype(jnp.bfloat16), "tp").astype(jnp.float32)
    return (mixed_float + added).astype(jnp.bfloat16)


PLANE = 4
MESH = pl.DeviceIdType.MESH


def remote(src, dst, send_sem, recv_sem, device):
    return pltpu.make_async_remote_copy(
        src_ref=src, dst_ref=dst, send_sem=send_sem, recv_sem=recv_sem,
        device_id=device, device_id_type=MESH,
    )


def last(a, b):
    return lax.dot_general(a, b, (((1,), (1,)), ((), ())), preferred_element_type=jnp.float32)


def folded(value):
    middle = value.shape[0] // 2
    return jnp.concatenate([value[:middle], value[middle:]], axis=1)


def unfolded(value):
    middle = value.shape[1] // 2
    return jnp.concatenate([value[:, :middle], value[:, middle:]], axis=0)


def add(a, b):
    return (a.astype(jnp.float32) + b.astype(jnp.float32)).astype(jnp.bfloat16)


def layer_kernel(
    line, size_a, size_b,
    bal_a, bal_b, resid_h, q1_h, k1_h, v1_h, q2_h, k2_h, v2_h, gain_a, gain_b, o1_h, o2_h,
    mlp_gain, up_h, down_h,
    out,
    resid, q1, k1, v1, q2, k2, v2, o1, o2, kv_own, q_own, kv_all, q_all, heads_out, heads_in,
    up_all, down_all, part, other_part, mixed, rows, hidden, terms, held, acc, below, above, total,
    fetch, kzs, kzr, qzs, qzr, kps, kpr, uzs, uzr, ups, upr, dzs, dzr, dps, dpr, hzs, hzr,
    sws, swr, rus, rds, rr, rcs, rcr, ts, tr, cus, cds, cbr, car, fs, fr,
):
    s = lax.axis_index("sp")
    c = lax.axis_index("tp")
    z = s // PLANE
    p = s % PLANE
    x = p % 2
    y = p // 2
    flip_x = y * 2 + 1 - x
    flip_y = (1 - y) * 2 + x
    near = (1 - c) * flip_x + c * flip_y
    side = (1 - c) * flip_y + c * flip_x
    far = (1 - y) * 2 + 1 - x
    to_near = (z * PLANE + near, c)
    to_side = (z * PLANE + side, c)
    to_core = (s, 1 - c)
    to_up = (s + PLANE, c)
    to_down = (s - PLANE, c)

    tokens = kv_own.shape[1]
    wide = gain_a.shape[1]
    deep = gain_b.shape[1]
    features = resid.shape[1]
    span = PLANE * tokens
    depth = up_h.shape[0]
    width = up_all.shape[1]
    half = tokens // 2
    part_depth = depth // 2
    count_all = line * PLANE
    piece = PLANE * depth

    def fetched(number, src, dst):
        return pltpu.make_async_copy(src, dst, fetch.at[number])

    def at_place(ref, number, size):
        return ref.at[pl.ds(pl.multiple_of(number * size, size), size)]

    def spot(name, h, number):
        if name == "up":
            return up_all.at[pl.ds(pl.multiple_of(number * depth + h * part_depth, part_depth), part_depth)]
        return down_all.at[pl.ds(pl.multiple_of((h * count_all + number) * part_depth, part_depth), part_depth)]

    small = [
        fetched(0, k1_h, k1), fetched(1, v1_h, v1), fetched(2, k2_h, k2), fetched(3, v2_h, v2),
        fetched(4, q1_h, q1), fetched(5, q2_h, q2),
    ]
    own_weights = {}
    for i, (name, source) in enumerate((("up", up_h), ("down", down_h))):
        for h in range(2):
            block = source.at[h * part_depth:(h + 1) * part_depth, pl.ds(pl.multiple_of(z * width, width), width)]
            own_weights[name, h] = fetched(6 + 2 * i + h, block, spot(name, h, s))
    large = [fetched(10, resid_h, resid), fetched(11, o1_h, o1), fetched(12, o2_h, o2)]
    for copy in small + list(own_weights.values()) + large:
        copy.start()

    barrier = pltpu.get_barrier_semaphore()
    peers = [to_near, to_side, to_core] + [(((z + j) % line) * PLANE + p, c) for j in range(1, line)]
    for device in peers:
        pl.semaphore_signal(barrier, inc=1, device_id=device, device_id_type=MESH)

    sends = []

    def send(*args):
        copy = remote(*args)
        copy.start()
        sends.append((None, copy))

    def send_if(condition, *args):
        copy = remote(*args)

        @pl.when(condition)
        def _():
            copy.start()

        sends.append((condition, copy))

    def arrived(block, sem):
        remote(block, block, fs.at[0], sem, to_core).wait_recv()

    for copy in small:
        copy.wait()
    count = tokens * line
    order = lax.broadcasted_iota(jnp.int32, (count, count), 0)
    place = lax.broadcasted_iota(jnp.int32, (count, count), 1)
    pick = jnp.where(place == (order % tokens) * line + order // tokens, 1.0, 0.0).astype(jnp.bfloat16)

    def by_head(value):
        moved = jnp.dot(pick, value, preferred_element_type=jnp.float32).astype(jnp.bfloat16)
        return moved.reshape(line, tokens, value.shape[1])

    row = lax.broadcasted_iota(jnp.int32, (tokens, tokens), 0)
    column = lax.broadcasted_iota(jnp.int32, (tokens, tokens), 1)
    same = jnp.where(row == column, 1.0, 0.0).astype(jnp.bfloat16)
    kv_own[:, :, 0:wide] = by_head(k1[...])
    kv_own[:, :, wide:2 * wide] = by_head(v1[...])
    for h in range(line):
        turned = last(same, jnp.concatenate([k2[h], v2[h]], axis=0))
        kv_own[h, :, 2 * wide:3 * wide] = turned.astype(jnp.bfloat16)
    q_own[:, 0:tokens, :] = by_head(q1[...])
    for h in range(line):
        q_own[h, tokens:, :] = folded(last(same, q2[h]).astype(jnp.bfloat16))
    pl.semaphore_wait(barrier, len(peers))

    def ahead(j):
        number = z
        bit = 1
        while bit <= j:
            if j & bit:
                number = number + bit * (1 - 2 * ((number // bit) % 2))
            bit *= 2
        return number

    behind = ahead

    def z_peer(j):
        return (ahead(j) * PLANE + p, c)

    mine = at_place(kv_all, s, tokens)
    for j in range(1, line):
        send(kv_own.at[ahead(j)], mine, kzs.at[j], kzr.at[j], z_peer(j))
    send(kv_own.at[z], mine, kps.at[0, 0], kpr.at[0, 0], to_near)
    send(kv_own.at[z], mine, kps.at[0, 1], kpr.at[0, 1], to_side)
    mine[...] = kv_own[z]
    q_all[z] = q_own[z]

    def push(name, h, j):
        source = up_h if name == "up" else down_h
        block = source.at[h * part_depth:(h + 1) * part_depth, pl.ds(pl.multiple_of(ahead(j) * width, width), width)]
        ss, sr = (uzs, uzr) if name == "up" else (dzs, dzr)
        send(block, spot(name, h, s), ss.at[h, j], sr.at[h, j], z_peer(j))

    def plane_sems(name):
        return (ups, upr) if name == "up" else (dps, dpr)

    def spread(name, h, j):
        block = spot(name, h, behind(j) * PLANE + p)
        if j:
            arrived(block, (uzr if name == "up" else dzr).at[h, j])
        else:
            own_weights[name, h].wait()
        ss, sr = plane_sems(name)
        send(block, block, ss.at[h, j, 0], sr.at[h, j, 0], to_near)
        send(block, block, ss.at[h, j, 1], sr.at[h, j, 1], to_side)

    def relay(name, h, j):
        block = spot(name, h, behind(j) * PLANE + near)
        ss, sr = plane_sems(name)
        arrived(block, sr.at[h, j, 0])
        send(block, block, ss.at[h, j, 2], sr.at[h, j, 2], to_side)

    def settle(name, h, j):
        ss, sr = plane_sems(name)
        for way, where in ((1, side), (2, far)):
            arrived(spot(name, h, behind(j) * PLANE + where), sr.at[h, j, way])

    done = []

    def flow(*items):
        for item in items:
            spread(*item)
            if done:
                relay(*done[-1])
            done.append(item)

    def ask():
        for j in range(1, line):
            send(q_own.at[ahead(j)], q_all.at[z], qzs.at[j], qzr.at[j], z_peer(j))

    def kv_spread(j):
        block = at_place(kv_all, behind(j) * PLANE + p, tokens)
        arrived(block, kzr.at[j])
        send(block, block, kps.at[j, 0], kpr.at[j, 0], to_near)
        send(block, block, kps.at[j, 1], kpr.at[j, 1], to_side)

    def kv_relay(j):
        block = at_place(kv_all, behind(j) * PLANE + near, tokens)
        arrived(block, kpr.at[j, 0])
        send(block, block, kps.at[j, 2], kpr.at[j, 2], to_side)

    kv_spread(1)
    kv_relay(0)

    kv_spread(2)
    ask()
    push("up", 0, 1)
    push("up", 1, 1)
    kv_relay(1)
    kv_spread(3)
    kv_relay(2)
    kv_relay(3)

    for j in range(line):
        for way, where in ((1, side), (2, far)):
            arrived(at_place(kv_all, behind(j) * PLANE + where, tokens), kpr.at[j, way])
    for j in range(1, line):
        arrived(q_all.at[behind(j)], qzr.at[j])
    flow(("up", 0, 0))
    push("up", 0, 2)
    push("up", 1, 2)

    lanes_a = lax.broadcasted_iota(jnp.int32, (tokens, wide), 1)
    lanes_b = lax.broadcasted_iota(jnp.int32, (tokens, deep), 1)
    line_rows = lax.broadcasted_iota(jnp.int32, (tokens, span), 0) + p * tokens
    visible = lax.broadcasted_iota(jnp.int32, (tokens, span), 1) <= line_rows

    def mix(queries, lanes, keys_at, values_at, size, b, keys_number):
        maps = []
        for m in range(2):
            chosen = (lanes >= m * size) & (lanes < (m + 1) * size)
            picked = jnp.where(chosen, queries, jnp.zeros_like(queries))
            scores = last(picked, kv_all[0:keys_number, keys_at]) * size ** (-0.5)
            tail_scores = jnp.where(visible, scores[:, keys_number - span:], -jnp.inf)
            if keys_number > span:
                scores = jnp.concatenate([scores[:, : keys_number - span], tail_scores], axis=1)
            else:
                scores = tail_scores
            powers = jnp.exp(scores - jnp.max(scores, axis=-1, keepdims=True))
            maps.append((powers, jnp.sum(powers, axis=-1, keepdims=True)))
        (e1, l1), (e2, l2) = maps
        mixing = (e1 * (1.0 / l1) - e2 * (b / l2)).astype(jnp.bfloat16)
        return jnp.dot(mixing, kv_all[0:keys_number, values_at], preferred_element_type=jnp.float32)

    def norm(value, gain):
        power = jnp.mean(value * value, axis=-1, keepdims=True)
        return (value * lax.rsqrt(power + EPSILON) * gain[...] * HEAD_SCALE).astype(jnp.bfloat16)

    def tile(j):
        number = (j + 1) * span
        first = mix(
            q_all[j, 0:tokens, :], lanes_a, slice(0, wide), slice(wide, 2 * wide), size_a, bal_a[z], number
        )
        heads_out[j, 0:tokens, :] = norm(first, gain_a)
        second = mix(
            unfolded(q_all[j, tokens:, :]), lanes_b, slice(2 * wide, 2 * wide + deep),
            slice(2 * wide, 3 * wide), size_b, bal_b[z], number,
        )
        heads_out[j, tokens:, :] = folded(norm(second[:, wide - deep:wide], gain_b))
        send_if(j != z, heads_out.at[j], heads_in.at[z], hzs.at[j], hzr.at[z], (j * PLANE + p, c))

    tile(3)

    tile(2)
    flow(("up", 1, 0))
    push("up", 0, 3)
    tile(1)

    tile(0)
    heads_in[z] = heads_out[z]
    push("up", 1, 3)
    push("down", 0, 1)
    flow(("down", 0, 0), ("down", 1, 0), ("up", 0, 1), ("up", 1, 1))
    for copy in large:
        copy.wait()
    for h in range(line):
        block = heads_in.at[h]

        @pl.when(h != z)
        def _():
            arrived(block, hzr.at[h])

    heads_first = jnp.concatenate([heads_in[h, 0:tokens, :] for h in range(line)], axis=1)
    heads_second = jnp.concatenate([unfolded(heads_in[h, tokens:, :]) for h in range(line)], axis=1)
    step = features // 4
    for n in range(4):
        at = slice(n * step, (n + 1) * step)
        value = jnp.dot(heads_first, o1[:, at], preferred_element_type=jnp.float32) + jnp.dot(
            heads_second, o2[:, at], preferred_element_type=jnp.float32
        )
        part[:, :, at] = value.astype(jnp.bfloat16).reshape(2, half, step)
    swap = remote(part.at[1 - c], other_part, sws.at[0], swr.at[0], to_core)
    swap.start()
    push("down", 0, 2)
    flow(("up", 0, 2))
    swap.wait()
    both = part[c].astype(jnp.float32) + other_part[...].astype(jnp.float32)
    mine_rows = pl.ds(pl.multiple_of(c * half, half), half)
    mixed[...] = (resid[mine_rows, :].astype(jnp.float32) + both).astype(jnp.bfloat16)
    whole = mixed[...].astype(jnp.float32)
    power = jnp.mean(whole * whole, axis=-1, keepdims=True)
    own_slot = at_place(rows, z * 2 + c, half)
    own_slot[...] = (whole * lax.rsqrt(power + EPSILON) * mlp_gain[...]).astype(jnp.bfloat16)

    send_if(z < line - 1, own_slot, own_slot, rus.at[0], rr.at[z], to_up)
    send_if(z > 0, own_slot, own_slot, rds.at[0], rr.at[z], to_down)
    send(own_slot, own_slot, rcs.at[0], rcr.at[z], to_core)

    def rows_pass(d):
        low = jnp.maximum(z - d, 0)
        high = jnp.minimum(z + d, line - 1)
        from_low = at_place(rows, low * 2 + c, half)
        from_high = at_place(rows, high * 2 + c, half)

        @pl.when(z >= d)
        def _():
            arrived(from_low, rr.at[low])

        send_if((z >= d) & (z < line - 1), from_low, from_low, rus.at[d], rr.at[low], to_up)
        send_if(z >= d, from_low, from_low, rcs.at[d], rcr.at[low], to_core)

        @pl.when(z + d < line)
        def _():
            arrived(from_high, rr.at[high])

        send_if((z + d < line) & (z > 0), from_high, from_high, rds.at[d], rr.at[high], to_down)
        send_if(z + d < line, from_high, from_high, rcs.at[line - 1 + d], rcr.at[high], to_core)

    flow(("up", 1, 2), ("up", 0, 3))
    rows_pass(1)
    push("down", 0, 3)
    push("down", 1, 1)
    flow(("up", 1, 3), ("down", 0, 1))
    rows_pass(2)
    for j in (2, 3):
        push("down", 1, j)
    flow(("down", 0, 2), ("down", 0, 3))
    rows_pass(3)
    flow(("down", 1, 1))
    lift = 256

    def raise_rows():
        for k in range(line):
            arrived(at_place(rows, k * 2 + 1 - c, half), rcr.at[k])
        for h in range(2):
            for j in range(line):
                settle("up", h, j)

        @pl.loop(0, width // lift)
        def _(n):
            at = pl.ds(pl.multiple_of(n * lift, lift), lift)
            lifted = jnp.maximum(jnp.dot(rows[...], up_all[:, at], preferred_element_type=jnp.float32), 0.0)
            hidden[:, at] = (lifted * lifted).astype(jnp.bfloat16)

    def chunk(k):
        at = slice(k * piece, (k + 1) * piece)
        value = last(hidden[...], down_all[k * piece:(k + 1) * piece, :]).astype(jnp.bfloat16)
        terms[:, :, :, at] = value.reshape(line, 2, half, piece)
        send(terms.at[:, 1 - c, :, at], held.at[:, :, at], ts.at[k], tr.at[k], to_core)

    ends = (z == 0) | (z == line - 1)
    inner = (z > 0) & (z < line - 1)

    def reduce(k, who):
        at = slice(k * piece, (k + 1) * piece)

        @pl.when(who)
        def _():
            arrived(held.at[:, :, at], tr.at[k])
            for zd in range(line):
                acc[zd, :, at] = add(terms[zd, c, :, at], held[zd, :, at])

        for d in range(line - 1, 0, -1):
            high = jnp.minimum(z + d, line - 1)
            block = below.at[high, :, at]

            @pl.when(who & (z + d < line) & (z > 0))
            def _():
                arrived(block, cbr.at[high, k])
                acc[high, :, at] = add(acc[high, :, at], below[high, :, at])

            send_if(who & (z + d < line), acc.at[high, :, at], block, cus.at[d, k], cbr.at[high, k], to_up)
            low = jnp.maximum(z - d, 0)
            block = above.at[low, :, at]

            @pl.when(who & (z >= d) & (z < line - 1))
            def _():
                arrived(block, car.at[low, k])
                acc[low, :, at] = add(acc[low, :, at], above[low, :, at])

            send_if(who & (z >= d), acc.at[low, :, at], block, cds.at[d, k], car.at[low, k], to_down)

    def finish(k):
        at = slice(k * piece, (k + 1) * piece)
        total[...] = acc[z, :, at].astype(jnp.float32)

        @pl.when(z > 0)
        def _():
            arrived(below.at[z, :, at], cbr.at[z, k])
            total[...] += below[z, :, at].astype(jnp.float32)

        @pl.when(z < line - 1)
        def _():
            arrived(above.at[z, :, at], car.at[z, k])
            total[...] += above[z, :, at].astype(jnp.float32)

        h = k // 2
        value = total[...]
        for i in range(piece // part_depth):
            number = (k % 2) * (piece // part_depth) + i
            to = slice(number * depth + h * part_depth, number * depth + (h + 1) * part_depth)
            term = value[:, i * part_depth:(i + 1) * part_depth]
            out[c, :, to] = (mixed[:, to].astype(jnp.float32) + term).astype(jnp.bfloat16)
        if h:
            to = slice((k % 2) * 2 * piece, (k % 2 + 1) * 2 * piece)
            send(out.at[c, :, to], out.at[c, :, to], fs.at[k % 2], fr.at[k % 2], to_core)

    raise_rows()
    flow(("down", 1, 2))
    for j in range(line):
        settle("down", 0, j)
    chunk(0)
    chunk(1)
    flow(("down", 1, 3))
    reduce(0, ends)
    reduce(1, ends)
    relay(*done[-1])
    for j in range(line):
        settle("down", 1, j)
    chunk(2)
    chunk(3)
    reduce(0, inner)
    reduce(1, inner)
    reduce(2, ends)
    reduce(3, ends)
    reduce(2, inner)
    reduce(3, inner)
    for k in range(4):
        finish(k)
    for k in range(2):
        to = slice(k * 2 * piece, (k + 1) * 2 * piece)
        arrived(out.at[1 - c, :, to], fr.at[k])
    for condition, copy in sends:
        if condition is None:
            copy.wait_send()
        else:

            @pl.when(condition)
            def _():
                copy.wait_send()


def layer(
    line, residual, q1, k1, v1, q2, k2, v2, bal_a, bal_b, gain_a, gain_b, o1, o2, mlp_gain, up, down
):
    tokens, features = residual.shape
    half = tokens // 2
    wide = v1.shape[1]
    n = line * PLANE
    width = up.shape[1] // line
    depth = up.shape[0]
    b16 = jnp.bfloat16
    dma = pltpu.SemaphoreType.DMA
    vmem = pl.BlockSpec(memory_space=pltpu.VMEM)
    smem = pl.BlockSpec(memory_space=pltpu.SMEM)
    any_ = pl.BlockSpec(memory_space=pl.ANY)

    def buffer(*shape):
        return pltpu.VMEM(shape, b16)

    return pl.pallas_call(
        functools.partial(layer_kernel, line, q1.shape[1] // 2, q2.shape[1] // 2),
        out_shape=jax.ShapeDtypeStruct((2, half, features), b16),
        in_specs=[smem, smem] + [any_] * 7 + [vmem, vmem, any_, any_, vmem, any_, any_],
        out_specs=vmem,
        scratch_shapes=[
            buffer(tokens, features), buffer(*q1.shape), buffer(*k1.shape), buffer(*v1.shape),
            buffer(*q2.shape), buffer(*k2.shape), buffer(*v2.shape), buffer(*o1.shape), buffer(*o2.shape),
            buffer(line, tokens, 3 * wide), buffer(line, tokens + half, wide),
            buffer(n * tokens, 3 * wide), buffer(line, tokens + half, wide),
            buffer(line, tokens + half, wide), buffer(line, tokens + half, wide),
            buffer(n * depth, width), buffer(n * depth, width),
            buffer(2, half, features), buffer(half, features), buffer(half, features),
            buffer(line * tokens, features), buffer(line * tokens, width),
            buffer(line, 2, half, features), buffer(line, half, features), buffer(line, half, features),
            buffer(line, half, features), buffer(line, half, features),
            pltpu.VMEM((half, PLANE * depth), jnp.float32),
            dma((13,)),
            dma((line,)), dma((line,)), dma((line,)), dma((line,)), dma((line, 3)), dma((line, 3)),
            dma((2, line)), dma((2, line)), dma((2, line, 3)), dma((2, line, 3)),
            dma((2, line)), dma((2, line)), dma((2, line, 3)), dma((2, line, 3)),
            dma((line,)), dma((line,)), dma((1,)), dma((1,)),
            dma((line,)), dma((line,)), dma((line,)), dma((2 * line - 1,)), dma((line,)),
            dma((line,)), dma((line,)), dma((line, line)), dma((line, line)),
            dma((line, line)), dma((line, line)), dma((2,)), dma((2,)),
        ],
        compiler_params=pltpu.CompilerParams(
            collective_id=0, has_side_effects=True, vmem_limit_bytes=60 * 1024 * 1024
        ),
    )(bal_a, bal_b, residual, q1, k1, v1, q2, k2, v2, gain_a, gain_b, o1, o2, mlp_gain, up, down)


def placed_body(
    residual, query_first, key_first, value_first, query_second, key_second, value_second,
    balance_first, balance_second, head_gain_first, head_gain_second, out_first, out_second,
    mlp_gain, up_weight, down_weight,
):
    tokens, line, _ = query_first.shape

    def flat(array):
        return array.reshape(tokens * line, array.shape[2])

    def turned(array):
        return array.transpose(1, 2, 0)

    out = layer(
        line, residual, flat(query_first), flat(key_first), flat(value_first), turned(query_second),
        turned(key_second), turned(value_second), balance_first, balance_second,
        head_gain_first[None, :], head_gain_second[None, :], out_first, out_second,
        mlp_gain[None, :], up_weight, down_weight,
    )
    return out.reshape(residual.shape)


def placed(mesh):
    ranks = mesh.shape["sp"]
    cores = mesh.shape["tp"]
    return cores == 2 and ranks % PLANE == 0


def choose(mesh):
    ranks = mesh.shape["sp"]

    def run(*arrays):
        query_first, query_second, value_second, value_first = arrays[1], arrays[4], arrays[6], arrays[3]
        fits = (
            placed(mesh)
            and ranks & (ranks - 1) == 0
            and query_first.shape[1] * PLANE == ranks
            and query_second.shape[1] == query_first.shape[1]
            and value_first.shape[2] == query_first.shape[2] == 128
            and query_second.shape[2] * 2 == value_second.shape[2] * 2 == query_first.shape[2]
            and query_first.shape[0] % 32 == 0
            and arrays[14].shape[1] % (128 * ranks) == 0
        )
        return (placed_body if fits else body)(*arrays)

    return run


def solution(mesh):
    in_specs = (
        P("sp", None),
        P("sp", "tp", None),
        P("sp", "tp", None),
        P("sp", "tp", None),
        P("sp", "tp", None),
        P("sp", "tp", None),
        P("sp", "tp", None),
        P("tp"),
        P("tp"),
        P(),
        P(),
        P("tp", None),
        P("tp", None),
        P(),
        P("sp", "tp"),
        P("sp", "tp"),
    )
    out_specs = P("sp", None)
    return jax.shard_map(choose(mesh), mesh=mesh, in_specs=in_specs, out_specs=out_specs, check_vma=False)
```

```python
import functools
import math

import jax
import jax.numpy as jnp
from jax import lax
from jax.experimental import pallas as pl
from jax.experimental.pallas import tpu as pltpu
from jax.sharding import PartitionSpec as P

DK_A = 64
DK_B = 32


EPSILON = 1e-06
HEAD_SCALE = 0.8


def attend(queries, keys, values, balance, gain, device, head_size):
    tokens = queries.shape[0]
    heads = queries.shape[1]
    seq = keys.shape[0]
    depth = values.shape[2]
    block = math.gcd(512, seq)
    scale = head_size ** (-0.5)
    query_maps = queries.reshape(tokens, heads, 2, head_size)
    key_maps = keys.reshape(seq, heads, 2, head_size)
    first_row = device * tokens
    positions = first_row + jnp.arange(tokens, dtype=jnp.int32)
    needed = (first_row + tokens + block - 1) // block

    def block_scores(number):
        start = number * block
        key_block = lax.dynamic_slice_in_dim(key_maps, start, block, 0)
        scores = (
            jnp.einsum("qhmd,khmd->hmqk", query_maps, key_block, preferred_element_type=jnp.float32)
            * scale
        )
        columns = start + jnp.arange(block, dtype=jnp.int32)
        visible = columns[None, :] <= positions[:, None]
        return (jnp.where(visible, scores, -jnp.inf), start)

    def statistics(number, carry):
        highest, total = carry
        scores, start = block_scores(number)
        fresh = jnp.maximum(highest, jnp.max(scores, axis=-1, keepdims=True))
        total = total * jnp.exp(highest - fresh) + jnp.sum(
            jnp.exp(scores - fresh), axis=-1, keepdims=True
        )
        return (fresh, total)

    start_high = jnp.full((heads, 2, tokens, 1), -jnp.inf, jnp.float32)
    start_total = jnp.zeros((heads, 2, tokens, 1), jnp.float32)
    highest, total = lax.fori_loop(0, needed, statistics, (start_high, start_total))

    def accumulate(number, result):
        scores, start = block_scores(number)
        probs = jnp.exp(scores - highest) / total
        mixed = (probs[:, 0] - balance[:, None, None] * probs[:, 1]).astype(jnp.bfloat16)
        value_block = lax.dynamic_slice_in_dim(values, start, block, 0)
        return result + jnp.einsum(
            "hqk,khe->qhe", mixed, value_block, preferred_element_type=jnp.float32
        )

    summed = lax.fori_loop(0, needed, accumulate, jnp.zeros((tokens, heads, depth), jnp.float32))
    power = jnp.mean(summed * summed, axis=-1, keepdims=True)
    normed = summed * lax.rsqrt(power + EPSILON) * gain * HEAD_SCALE
    return normed.astype(jnp.bfloat16).reshape(tokens, heads * depth)


def body(
    residual,
    query_first,
    key_first,
    value_first,
    query_second,
    key_second,
    value_second,
    balance_first,
    balance_second,
    head_gain_first,
    head_gain_second,
    out_first,
    out_second,
    mlp_gain,
    up_weight,
    down_weight,
):
    device = lax.axis_index("sp")
    keys_first, values_first, keys_second, values_second = (
        lax.all_gather(key_first, "sp", axis=0, tiled=True),
        lax.all_gather(value_first, "sp", axis=0, tiled=True),
        lax.all_gather(key_second, "sp", axis=0, tiled=True),
        lax.all_gather(value_second, "sp", axis=0, tiled=True),
    )
    heads_first = attend(
        query_first, keys_first, values_first, balance_first, head_gain_first, device, DK_A
    )
    heads_second = attend(
        query_second, keys_second, values_second, balance_second, head_gain_second, device, DK_B
    )
    head_term = jnp.dot(heads_first, out_first, preferred_element_type=jnp.float32) + jnp.dot(
        heads_second, out_second, preferred_element_type=jnp.float32
    )
    head_total = lax.psum(head_term.astype(jnp.bfloat16), "tp").astype(jnp.float32)
    mixed = (residual.astype(jnp.float32) + head_total).astype(jnp.bfloat16)
    mixed_float = mixed.astype(jnp.float32)
    power = jnp.mean(mixed_float * mixed_float, axis=-1, keepdims=True)
    normed = (mixed_float * lax.rsqrt(power + EPSILON) * mlp_gain).astype(jnp.bfloat16)
    up_whole, down_whole = (
        lax.all_gather(up_weight, "sp", axis=0, tiled=True),
        lax.all_gather(down_weight, "sp", axis=0, tiled=True),
    )
    lifted = jnp.dot(normed, up_whole, preferred_element_type=jnp.float32)
    active = jax.nn.relu(lifted)
    hidden = (active * active).astype(jnp.bfloat16)
    down_term = lax.dot_general(
        hidden, down_whole, (((1,), (1,)), ((), ())), preferred_element_type=jnp.float32
    )
    added = lax.psum(down_term.astype(jnp.bfloat16), "tp").astype(jnp.float32)
    return (mixed_float + added).astype(jnp.bfloat16)


PLANE = 4
MESH = pl.DeviceIdType.MESH


def remote(src, dst, send_sem, recv_sem, device):
    return pltpu.make_async_remote_copy(
        src_ref=src, dst_ref=dst, send_sem=send_sem, recv_sem=recv_sem,
        device_id=device, device_id_type=MESH,
    )


def last(a, b):
    return lax.dot_general(a, b, (((1,), (1,)), ((), ())), preferred_element_type=jnp.float32)


def folded(value):
    middle = value.shape[0] // 2
    return jnp.concatenate([value[:middle], value[middle:]], axis=1)


def unfolded(value):
    middle = value.shape[1] // 2
    return jnp.concatenate([value[:, :middle], value[:, middle:]], axis=0)


def add(a, b):
    return (a.astype(jnp.float32) + b.astype(jnp.float32)).astype(jnp.bfloat16)


def layer_kernel(
    line, size_a, size_b,
    bal_a, bal_b, resid_h, q1_h, k1_h, v1_h, q2_h, k2_h, v2_h, gain_a, gain_b, o1_h, o2_h,
    mlp_gain, up_h, down_h,
    out,
    resid, q1, k1, v1, q2, k2, v2, o1, o2, kv_own, q_own, kv_all, q_all, heads_out, heads_in,
    up_all, down_all, part, other_part, mixed, rows, hidden, terms, held, acc, relays, from_mate, from_across, result,
    fetch, kzs, kzr, qzs, qzr, kps, kpr, uzs, uzr, ups, upr, dzs, dzr, dps, dpr, hzs, hzr,
    sws, swr, rus, rds, rr, rcs, rcr, ts, tr, cus, cds, cbr, car, fs, fr,
):
    s = lax.axis_index("sp")
    c = lax.axis_index("tp")
    z = s // PLANE
    p = s % PLANE
    x = p % 2
    y = p // 2
    flip_x = y * 2 + 1 - x
    flip_y = (1 - y) * 2 + x
    near = (1 - c) * flip_x + c * flip_y
    side = (1 - c) * flip_y + c * flip_x
    far = (1 - y) * 2 + 1 - x
    to_near = (z * PLANE + near, c)
    to_side = (z * PLANE + side, c)
    to_core = (s, 1 - c)
    to_up = (s + PLANE, c)
    to_down = (s - PLANE, c)

    tokens = kv_own.shape[1]
    wide = gain_a.shape[1]
    deep = gain_b.shape[1]
    features = resid.shape[1]
    span = PLANE * tokens
    depth = up_h.shape[0]
    width = up_all.shape[1]
    half = tokens // 2
    stages = {"up": 2, "down": line}
    share = {name: depth // number for name, number in stages.items()}
    count_all = line * PLANE
    piece = PLANE * depth

    def fetched(number, src, dst):
        return pltpu.make_async_copy(src, dst, fetch.at[number])

    def at_place(ref, number, size):
        return ref.at[pl.ds(pl.multiple_of(number * size, size), size)]

    def spot(name, h, number):
        size = share[name]
        if name == "up":
            return up_all.at[pl.ds(pl.multiple_of(number * depth + h * size, size), size)]
        return down_all.at[pl.ds(pl.multiple_of((h * count_all + number) * size, size), size)]

    small = [
        fetched(0, k1_h, k1), fetched(1, v1_h, v1), fetched(2, k2_h, k2), fetched(3, v2_h, v2),
        fetched(4, q1_h, q1), fetched(5, q2_h, q2),
    ]
    own_weights = {}
    for i, (name, source) in enumerate((("up", up_h), ("down", down_h))):
        for h in range(stages[name]):
            rows_at = slice(h * share[name], (h + 1) * share[name])
            block = source.at[rows_at, pl.ds(pl.multiple_of(z * width, width), width)]
            own_weights[name, h] = fetched(9 + 2 * i + h, block, spot(name, h, s))
    large = [fetched(6, resid_h, resid), fetched(7, o1_h, o1), fetched(8, o2_h, o2)]
    for copy in small + list(own_weights.values()) + large:
        copy.start()

    barrier = pltpu.get_barrier_semaphore()
    peers = [to_near, to_side, to_core] + [(((z + j) % line) * PLANE + p, c) for j in range(1, line)]
    for device in peers:
        pl.semaphore_signal(barrier, inc=1, device_id=device, device_id_type=MESH)

    sends = []

    def send(*args):
        copy = remote(*args)
        copy.start()
        sends.append((None, copy))

    def send_if(condition, *args):
        copy = remote(*args)

        @pl.when(condition)
        def _():
            copy.start()

        sends.append((condition, copy))

    def arrived(block, sem):
        remote(block, block, fs.at[0], sem, to_core).wait_recv()

    for copy in small:
        copy.wait()
    count = tokens * line
    order = lax.broadcasted_iota(jnp.int32, (count, count), 0)
    place = lax.broadcasted_iota(jnp.int32, (count, count), 1)
    pick = jnp.where(place == (order % tokens) * line + order // tokens, 1.0, 0.0).astype(jnp.bfloat16)

    def by_head(value):
        moved = jnp.dot(pick, value, preferred_element_type=jnp.float32).astype(jnp.bfloat16)
        return moved.reshape(line, tokens, value.shape[1])

    row = lax.broadcasted_iota(jnp.int32, (tokens, tokens), 0)
    column = lax.broadcasted_iota(jnp.int32, (tokens, tokens), 1)
    same = jnp.where(row == column, 1.0, 0.0).astype(jnp.bfloat16)
    kv_own[:, :, 0:wide] = by_head(k1[...])
    kv_own[:, :, wide:2 * wide] = by_head(v1[...])
    for h in range(line):
        turned = last(same, jnp.concatenate([k2[h], v2[h]], axis=0))
        kv_own[h, :, 2 * wide:3 * wide] = turned.astype(jnp.bfloat16)
    q_own[:, 0:tokens, :] = by_head(q1[...])
    for h in range(line):
        q_own[h, tokens:, :] = folded(last(same, q2[h]).astype(jnp.bfloat16))
    pl.semaphore_wait(barrier, len(peers))

    def ahead(j):
        number = z
        bit = 1
        while bit <= j:
            if j & bit:
                number = number + bit * (1 - 2 * ((number // bit) % 2))
            bit *= 2
        return number

    behind = ahead

    def z_peer(j):
        return (ahead(j) * PLANE + p, c)

    mine = at_place(kv_all, s, tokens)
    for j in range(1, line):
        send(kv_own.at[ahead(j)], mine, kzs.at[j], kzr.at[j], z_peer(j))
    send(kv_own.at[z], mine, kps.at[0, 0], kpr.at[0, 0], to_near)
    send(kv_own.at[z], mine, kps.at[0, 1], kpr.at[0, 1], to_side)
    mine[...] = kv_own[z]
    q_all[z] = q_own[z]

    def push(name, h, j):
        source = up_h if name == "up" else down_h
        rows_at = slice(h * share[name], (h + 1) * share[name])
        block = source.at[rows_at, pl.ds(pl.multiple_of(ahead(j) * width, width), width)]
        ss, sr = (uzs, uzr) if name == "up" else (dzs, dzr)
        send(block, spot(name, h, s), ss.at[h, j], sr.at[h, j], z_peer(j))

    def plane_sems(name):
        return (ups, upr) if name == "up" else (dps, dpr)

    def spread(name, h, j):
        block = spot(name, h, behind(j) * PLANE + p)
        if j:
            arrived(block, (uzr if name == "up" else dzr).at[h, j])
        else:
            own_weights[name, h].wait()
        ss, sr = plane_sems(name)
        send(block, block, ss.at[h, j, 0], sr.at[h, j, 0], to_near)
        send(block, block, ss.at[h, j, 1], sr.at[h, j, 1], to_side)

    def relay(name, h, j):
        block = spot(name, h, behind(j) * PLANE + near)
        ss, sr = plane_sems(name)
        arrived(block, sr.at[h, j, 0])
        send(block, block, ss.at[h, j, 2], sr.at[h, j, 2], to_side)

    def settle(name, h, j):
        ss, sr = plane_sems(name)
        for way, where in ((1, side), (2, far)):
            arrived(spot(name, h, behind(j) * PLANE + where), sr.at[h, j, way])

    done = []
    lag = 2

    def flow(*items):
        for item in items:
            spread(*item)
            if len(done) >= lag:
                relay(*done[-lag])
            done.append(item)

    def drain():
        for item in done[-lag:]:
            relay(*item)

    def ask():
        for j in range(1, line):
            send(q_own.at[ahead(j)], q_all.at[z], qzs.at[j], qzr.at[j], z_peer(j))

    def kv_spread(j):
        block = at_place(kv_all, behind(j) * PLANE + p, tokens)
        arrived(block, kzr.at[j])
        send(block, block, kps.at[j, 0], kpr.at[j, 0], to_near)
        send(block, block, kps.at[j, 1], kpr.at[j, 1], to_side)

    def kv_relay(j):
        block = at_place(kv_all, behind(j) * PLANE + near, tokens)
        arrived(block, kpr.at[j, 0])
        send(block, block, kps.at[j, 2], kpr.at[j, 2], to_side)

    kv_spread(1)
    kv_relay(0)
    kv_spread(2)
    kv_relay(1)
    kv_spread(3)
    push("down", 2, 3)
    ask()
    push("up", 0, 1)
    push("up", 1, 1)
    push("down", 3, 3)
    kv_relay(2)
    kv_relay(3)
    for j in range(line):
        for way, where in ((1, side), (2, far)):
            arrived(at_place(kv_all, behind(j) * PLANE + where, tokens), kpr.at[j, way])
    for j in range(1, line):
        arrived(q_all.at[behind(j)], qzr.at[j])
    flow(("up", 0, 0))
    push("up", 0, 2)

    lanes_a = lax.broadcasted_iota(jnp.int32, (tokens, wide), 1)
    lanes_b = lax.broadcasted_iota(jnp.int32, (tokens, deep), 1)
    line_rows = lax.broadcasted_iota(jnp.int32, (2 * tokens, span), 0) % tokens + p * tokens
    visible = lax.broadcasted_iota(jnp.int32, (2 * tokens, span), 1) <= line_rows

    def mix(queries, lanes, keys_at, values_at, size, b, keys_number):
        zeros = jnp.zeros_like(queries)
        picked = jnp.concatenate(
            [jnp.where(lanes < size, queries, zeros), jnp.where(lanes < size, zeros, queries)], axis=0
        )
        scores = last(picked, kv_all[0:keys_number, keys_at])
        tail_scores = jnp.where(visible, scores[:, keys_number - span:], -jnp.inf)
        if keys_number > span:
            scores = jnp.concatenate([scores[:, : keys_number - span], tail_scores], axis=1)
        else:
            scores = tail_scores
        gaps = scores - jnp.max(scores, axis=-1, keepdims=True)
        powers = jnp.exp2(gaps * (size ** (-0.5) * math.log2(math.e)))
        sums = jnp.sum(powers, axis=-1, keepdims=True)
        both = jnp.dot(
            powers.astype(jnp.bfloat16), kv_all[0:keys_number, values_at], preferred_element_type=jnp.float32
        )
        return both[:tokens] * (1.0 / sums[:tokens]) - both[tokens:] * (b / sums[tokens:])

    def norm(value, gain):
        power = jnp.mean(value * value, axis=-1, keepdims=True)
        return (value * lax.rsqrt(power + EPSILON) * gain[...] * HEAD_SCALE).astype(jnp.bfloat16)

    def tile(j):
        number = (j + 1) * span
        first = mix(
            q_all[j, 0:tokens, :], lanes_a, slice(0, wide), slice(wide, 2 * wide), size_a, bal_a[z], number
        )
        heads_out[j, 0:tokens, :] = norm(first, gain_a)
        second = mix(
            unfolded(q_all[j, tokens:, :]), lanes_b, slice(2 * wide, 2 * wide + deep),
            slice(2 * wide, 3 * wide), size_b, bal_b[z], number,
        )
        heads_out[j, tokens:, :] = folded(norm(second[:, wide - deep:wide], gain_b))
        send_if(j != z, heads_out.at[j], heads_in.at[z], hzs.at[j], hzr.at[z], (j * PLANE + p, c))

    tile(3)

    tile(2)
    flow(("up", 1, 0))
    push("up", 1, 2)
    tile(1)

    tile(0)
    heads_in[z] = heads_out[z]
    push("up", 0, 3)
    push("down", 0, 1)
    push("down", 1, 1)
    flow(("down", 0, 0))
    flow(("down", 1, 0))
    flow(("down", 2, 0))
    flow(("down", 3, 0))
    push("up", 1, 3)
    flow(("up", 0, 1))
    flow(("up", 1, 1))
    for copy in large:
        copy.wait()
    for h in range(line):
        block = heads_in.at[h]

        @pl.when(h != z)
        def _():
            arrived(block, hzr.at[h])

    heads_first = jnp.concatenate([heads_in[h, 0:tokens, :] for h in range(line)], axis=1)
    heads_second = jnp.concatenate([unfolded(heads_in[h, tokens:, :]) for h in range(line)], axis=1)
    step = features // 4
    for n in range(4):
        at = slice(n * step, (n + 1) * step)
        value = jnp.dot(heads_first, o1[:, at], preferred_element_type=jnp.float32) + jnp.dot(
            heads_second, o2[:, at], preferred_element_type=jnp.float32
        )
        part[:, :, at] = value.astype(jnp.bfloat16).reshape(2, half, step)
    swap = remote(part.at[1 - c], other_part, sws.at[0], swr.at[0], to_core)
    swap.start()
    flow(("up", 0, 2))
    swap.wait()
    both = part[c].astype(jnp.float32) + other_part[...].astype(jnp.float32)
    mine_rows = pl.ds(pl.multiple_of(c * half, half), half)
    mixed[...] = (resid[mine_rows, :].astype(jnp.float32) + both).astype(jnp.bfloat16)
    whole = mixed[...].astype(jnp.float32)
    power = jnp.mean(whole * whole, axis=-1, keepdims=True)
    own_slot = at_place(rows, z * 2 + c, half)
    own_slot[...] = (whole * lax.rsqrt(power + EPSILON) * mlp_gain[...]).astype(jnp.bfloat16)

    send_if(z < line - 1, own_slot, own_slot, rus.at[0], rr.at[z], to_up)
    send_if(z > 0, own_slot, own_slot, rds.at[0], rr.at[z], to_down)
    send(own_slot, own_slot, rcs.at[0], rcr.at[z], to_core)

    def rows_low(d):
        low = jnp.maximum(z - d, 0)
        from_low = at_place(rows, low * 2 + c, half)

        @pl.when(z >= d)
        def _():
            arrived(from_low, rr.at[low])

        send_if((z >= d) & (z < line - 1), from_low, from_low, rus.at[d], rr.at[low], to_up)
        send_if(z >= d, from_low, from_low, rcs.at[d], rcr.at[low], to_core)

    def rows_high(d):
        high = jnp.minimum(z + d, line - 1)
        from_high = at_place(rows, high * 2 + c, half)

        @pl.when(z + d < line)
        def _():
            arrived(from_high, rr.at[high])

        send_if((z + d < line) & (z > 0), from_high, from_high, rds.at[d], rr.at[high], to_down)
        send_if(z + d < line, from_high, from_high, rcs.at[line - 1 + d], rcr.at[high], to_core)

    flow(("up", 1, 2))
    flow(("up", 0, 3))
    push("down", 0, 2)
    push("down", 1, 2)
    rows_low(1)
    rows_high(1)
    push("down", 0, 3)
    push("down", 1, 3)
    push("down", 2, 1)
    flow(("up", 1, 3))
    flow(("down", 0, 1))
    flow(("down", 1, 1))
    push("down", 3, 1)
    rows_low(2)
    rows_high(2)
    flow(("down", 1, 2))
    push("down", 2, 2)
    push("down", 3, 2)
    flow(("down", 0, 2))
    flow(("down", 0, 3))
    flow(("down", 1, 3))
    rows_low(3)
    rows_high(3)
    flow(("down", 2, 1))
    flow(("down", 3, 1))
    lift = 256

    def raise_rows():
        for k in range(line):
            arrived(at_place(rows, k * 2 + 1 - c, half), rcr.at[k])
        for h in range(2):
            for j in range(line):
                settle("up", h, j)

        @pl.loop(0, width // lift)
        def _(n):
            at = pl.ds(pl.multiple_of(n * lift, lift), lift)
            lifted = jnp.maximum(jnp.dot(rows[...], up_all[:, at], preferred_element_type=jnp.float32), 0.0)
            hidden[:, at] = (lifted * lifted).astype(jnp.bfloat16)

    def chunk(k):
        at = slice(k * piece, (k + 1) * piece)
        value = last(hidden[...], down_all[k * piece:(k + 1) * piece, :]).astype(jnp.bfloat16)
        terms[:, :, :, at] = value.reshape(line, 2, half, piece)
        send(terms.at[:, 1 - c, :, at], held.at[:, :, at], ts.at[k], tr.at[k], to_core)

    upper = z // 2
    ends = (z == 0) | (z == line - 1)
    inner = (z > 0) & (z < line - 1)
    mate = ahead(1)
    to_mate = (mate * PLANE + p, c)
    across = [2 - upper, (1 - upper) * (line - 1)]

    def combine(k):
        at = slice(k * piece, (k + 1) * piece)
        arrived(held.at[:, :, at], tr.at[k])
        for zd in range(line):
            acc[zd, :, at] = add(terms[zd, c, :, at], held[zd, :, at])
        for r in (1, 0):
            block = acc.at[across[r], :, at]
            send_if(ends, block, relays.at[r, :, at], cus.at[r, k], cbr.at[r, k], to_mate)
        send(acc.at[mate, :, at], from_mate.at[:, at], cds.at[0, k], car.at[0, k], to_mate)

    def cross(k):
        at = slice(k * piece, (k + 1) * piece)
        for r in (1, 0):
            block = acc.at[across[r], :, at]

            @pl.when(inner)
            def _():
                arrived(relays.at[r, :, at], cbr.at[r, k])
                block[...] = add(block[...], relays[r, :, at])

            send_if(
                inner, block, from_across.at[:, at], cus.at[2 + r, k], car.at[1, k],
                (across[r] * PLANE + p, c),
            )

    def finish(k):
        at = slice(k * piece, (k + 1) * piece)
        arrived(from_mate.at[:, at], car.at[0, k])
        arrived(from_across.at[:, at], car.at[1, k])
        value = acc[z, :, at].astype(jnp.float32) + from_mate[:, at].astype(jnp.float32)
        value = value + from_across[:, at].astype(jnp.float32)
        size = share["down"]
        for i in range(count_all):
            to = slice(i * depth + k * size, i * depth + (k + 1) * size)
            term = value[:, i * size:(i + 1) * size]
            result[:, to] = (mixed[:, to].astype(jnp.float32) + term).astype(jnp.bfloat16)
        if k == line - 1:
            send(result, out.at[c], fs.at[0], fr.at[0], to_core)
            fetched(10 + line, result, out.at[c]).start()

    raise_rows()
    flow(("down", 2, 2))
    for j in range(line):
        settle("down", 0, j)
    chunk(0)
    for j in range(line):
        settle("down", 1, j)
    chunk(1)
    flow(("down", 2, 3))
    combine(0)
    combine(1)
    flow(("down", 3, 2))
    flow(("down", 3, 3))
    drain()
    cross(0)
    for j in range(line):
        settle("down", 2, j)
    chunk(2)
    combine(2)
    cross(1)
    for j in range(line):
        settle("down", 3, j)
    chunk(3)
    combine(3)
    finish(0)
    finish(1)
    cross(2)
    cross(3)
    finish(2)
    finish(3)
    arrived(out.at[1 - c], fr.at[0])
    fetched(10 + line, result, out.at[c]).wait()
    for condition, copy in sends:
        if condition is None:
            copy.wait_send()
        else:

            @pl.when(condition)
            def _():
                copy.wait_send()


def layer(
    line, residual, q1, k1, v1, q2, k2, v2, bal_a, bal_b, gain_a, gain_b, o1, o2, mlp_gain, up, down
):
    tokens, features = residual.shape
    half = tokens // 2
    wide = v1.shape[1]
    n = line * PLANE
    width = up.shape[1] // line
    depth = up.shape[0]
    b16 = jnp.bfloat16
    dma = pltpu.SemaphoreType.DMA
    vmem = pl.BlockSpec(memory_space=pltpu.VMEM)
    smem = pl.BlockSpec(memory_space=pltpu.SMEM)
    any_ = pl.BlockSpec(memory_space=pl.ANY)

    def buffer(*shape):
        return pltpu.VMEM(shape, b16)

    return pl.pallas_call(
        functools.partial(layer_kernel, line, q1.shape[1] // 2, q2.shape[1] // 2),
        out_shape=jax.ShapeDtypeStruct((2, half, features), b16),
        in_specs=[smem, smem] + [any_] * 7 + [vmem, vmem, any_, any_, vmem, any_, any_],
        out_specs=any_,
        scratch_shapes=[
            buffer(tokens, features), buffer(*q1.shape), buffer(*k1.shape), buffer(*v1.shape),
            buffer(*q2.shape), buffer(*k2.shape), buffer(*v2.shape), buffer(*o1.shape), buffer(*o2.shape),
            buffer(line, tokens, 3 * wide), buffer(line, tokens + half, wide),
            buffer(n * tokens, 3 * wide), buffer(line, tokens + half, wide),
            buffer(line, tokens + half, wide), buffer(line, tokens + half, wide),
            buffer(n * depth, width), buffer(n * depth, width),
            buffer(2, half, features), buffer(half, features), buffer(half, features),
            buffer(line * tokens, features), buffer(line * tokens, width),
            buffer(line, 2, half, features), buffer(line, half, features), buffer(line, half, features),
            buffer(2, half, features), buffer(half, features), buffer(half, features), buffer(half, features),
            dma((11 + line,)),
            dma((line,)), dma((line,)), dma((line,)), dma((line,)), dma((line, 3)), dma((line, 3)),
            dma((2, line)), dma((2, line)), dma((2, line, 3)), dma((2, line, 3)),
            dma((line, line)), dma((line, line)), dma((line, line, 3)), dma((line, line, 3)),
            dma((line,)), dma((line,)), dma((1,)), dma((1,)),
            dma((line,)), dma((line,)), dma((line,)), dma((2 * line - 1,)), dma((line,)),
            dma((line,)), dma((line,)), dma((line, line)), dma((1, line)),
            dma((2, line)), dma((2, line)), dma((1,)), dma((1,)),
        ],
        compiler_params=pltpu.CompilerParams(
            collective_id=0, has_side_effects=True, vmem_limit_bytes=60 * 1024 * 1024
        ),
    )(bal_a, bal_b, residual, q1, k1, v1, q2, k2, v2, gain_a, gain_b, o1, o2, mlp_gain, up, down)


def placed_body(
    residual, query_first, key_first, value_first, query_second, key_second, value_second,
    balance_first, balance_second, head_gain_first, head_gain_second, out_first, out_second,
    mlp_gain, up_weight, down_weight,
):
    tokens, line, _ = query_first.shape

    def flat(array):
        return array.reshape(tokens * line, array.shape[2])

    def turned(array):
        return array.transpose(1, 2, 0)

    out = layer(
        line, residual, flat(query_first), flat(key_first), flat(value_first), turned(query_second),
        turned(key_second), turned(value_second), balance_first, balance_second,
        head_gain_first[None, :], head_gain_second[None, :], out_first, out_second,
        mlp_gain[None, :], up_weight, down_weight,
    )
    return out.reshape(residual.shape)


def placed(mesh):
    ranks = mesh.shape["sp"]
    cores = mesh.shape["tp"]
    return cores == 2 and ranks % PLANE == 0


def choose(mesh):
    ranks = mesh.shape["sp"]

    def run(*arrays):
        query_first, query_second, value_second, value_first = arrays[1], arrays[4], arrays[6], arrays[3]
        fits = (
            placed(mesh)
            and ranks & (ranks - 1) == 0
            and query_first.shape[1] * PLANE == ranks
            and query_second.shape[1] == query_first.shape[1]
            and value_first.shape[2] == query_first.shape[2] == 128
            and query_second.shape[2] * 2 == value_second.shape[2] * 2 == query_first.shape[2]
            and query_first.shape[0] % 32 == 0
            and arrays[14].shape[1] % (128 * ranks) == 0
        )
        return (placed_body if fits else body)(*arrays)

    return run


def solution(mesh):
    in_specs = (
        P("sp", None),
        P("sp", "tp", None),
        P("sp", "tp", None),
        P("sp", "tp", None),
        P("sp", "tp", None),
        P("sp", "tp", None),
        P("sp", "tp", None),
        P("tp"),
        P("tp"),
        P(),
        P(),
        P("tp", None),
        P("tp", None),
        P(),
        P("sp", "tp"),
        P("sp", "tp"),
    )
    out_specs = P("sp", None)
    return jax.shard_map(choose(mesh), mesh=mesh, in_specs=in_specs, out_specs=out_specs, check_vma=False)
```

```python
import functools
import math

import jax
import jax.numpy as jnp
from jax import lax
from jax.experimental import pallas as pl
from jax.experimental.pallas import tpu as pltpu
from jax.sharding import PartitionSpec as P

DK_A = 64
DK_B = 32


EPSILON = 1e-06
HEAD_SCALE = 0.8


def attend(queries, keys, values, balance, gain, device, head_size):
    tokens = queries.shape[0]
    heads = queries.shape[1]
    seq = keys.shape[0]
    depth = values.shape[2]
    block = math.gcd(512, seq)
    scale = head_size ** (-0.5)
    query_maps = queries.reshape(tokens, heads, 2, head_size)
    key_maps = keys.reshape(seq, heads, 2, head_size)
    first_row = device * tokens
    positions = first_row + jnp.arange(tokens, dtype=jnp.int32)
    needed = (first_row + tokens + block - 1) // block

    def block_scores(number):
        start = number * block
        key_block = lax.dynamic_slice_in_dim(key_maps, start, block, 0)
        scores = (
            jnp.einsum("qhmd,khmd->hmqk", query_maps, key_block, preferred_element_type=jnp.float32)
            * scale
        )
        columns = start + jnp.arange(block, dtype=jnp.int32)
        visible = columns[None, :] <= positions[:, None]
        return (jnp.where(visible, scores, -jnp.inf), start)

    def statistics(number, carry):
        highest, total = carry
        scores, start = block_scores(number)
        fresh = jnp.maximum(highest, jnp.max(scores, axis=-1, keepdims=True))
        total = total * jnp.exp(highest - fresh) + jnp.sum(
            jnp.exp(scores - fresh), axis=-1, keepdims=True
        )
        return (fresh, total)

    start_high = jnp.full((heads, 2, tokens, 1), -jnp.inf, jnp.float32)
    start_total = jnp.zeros((heads, 2, tokens, 1), jnp.float32)
    highest, total = lax.fori_loop(0, needed, statistics, (start_high, start_total))

    def accumulate(number, result):
        scores, start = block_scores(number)
        probs = jnp.exp(scores - highest) / total
        mixed = (probs[:, 0] - balance[:, None, None] * probs[:, 1]).astype(jnp.bfloat16)
        value_block = lax.dynamic_slice_in_dim(values, start, block, 0)
        return result + jnp.einsum(
            "hqk,khe->qhe", mixed, value_block, preferred_element_type=jnp.float32
        )

    summed = lax.fori_loop(0, needed, accumulate, jnp.zeros((tokens, heads, depth), jnp.float32))
    power = jnp.mean(summed * summed, axis=-1, keepdims=True)
    normed = summed * lax.rsqrt(power + EPSILON) * gain * HEAD_SCALE
    return normed.astype(jnp.bfloat16).reshape(tokens, heads * depth)


def body(
    residual,
    query_first,
    key_first,
    value_first,
    query_second,
    key_second,
    value_second,
    balance_first,
    balance_second,
    head_gain_first,
    head_gain_second,
    out_first,
    out_second,
    mlp_gain,
    up_weight,
    down_weight,
):
    device = lax.axis_index("sp")
    keys_first, values_first, keys_second, values_second = (
        lax.all_gather(key_first, "sp", axis=0, tiled=True),
        lax.all_gather(value_first, "sp", axis=0, tiled=True),
        lax.all_gather(key_second, "sp", axis=0, tiled=True),
        lax.all_gather(value_second, "sp", axis=0, tiled=True),
    )
    heads_first = attend(
        query_first, keys_first, values_first, balance_first, head_gain_first, device, DK_A
    )
    heads_second = attend(
        query_second, keys_second, values_second, balance_second, head_gain_second, device, DK_B
    )
    head_term = jnp.dot(heads_first, out_first, preferred_element_type=jnp.float32) + jnp.dot(
        heads_second, out_second, preferred_element_type=jnp.float32
    )
    head_total = lax.psum(head_term.astype(jnp.bfloat16), "tp").astype(jnp.float32)
    mixed = (residual.astype(jnp.float32) + head_total).astype(jnp.bfloat16)
    mixed_float = mixed.astype(jnp.float32)
    power = jnp.mean(mixed_float * mixed_float, axis=-1, keepdims=True)
    normed = (mixed_float * lax.rsqrt(power + EPSILON) * mlp_gain).astype(jnp.bfloat16)
    up_whole, down_whole = (
        lax.all_gather(up_weight, "sp", axis=0, tiled=True),
        lax.all_gather(down_weight, "sp", axis=0, tiled=True),
    )
    lifted = jnp.dot(normed, up_whole, preferred_element_type=jnp.float32)
    active = jax.nn.relu(lifted)
    hidden = (active * active).astype(jnp.bfloat16)
    down_term = lax.dot_general(
        hidden, down_whole, (((1,), (1,)), ((), ())), preferred_element_type=jnp.float32
    )
    added = lax.psum(down_term.astype(jnp.bfloat16), "tp").astype(jnp.float32)
    return (mixed_float + added).astype(jnp.bfloat16)


PLANE = 4
MESH = pl.DeviceIdType.MESH


def remote(src, dst, send_sem, recv_sem, device):
    return pltpu.make_async_remote_copy(
        src_ref=src, dst_ref=dst, send_sem=send_sem, recv_sem=recv_sem,
        device_id=device, device_id_type=MESH,
    )


def last(a, b):
    return lax.dot_general(a, b, (((1,), (1,)), ((), ())), preferred_element_type=jnp.float32)


def folded(value):
    middle = value.shape[0] // 2
    return jnp.concatenate([value[:middle], value[middle:]], axis=1)


def unfolded(value):
    middle = value.shape[1] // 2
    return jnp.concatenate([value[:, :middle], value[:, middle:]], axis=0)


def add(a, b):
    return (a.astype(jnp.float32) + b.astype(jnp.float32)).astype(jnp.bfloat16)


def layer_kernel(
    line, size_a, size_b,
    bal_a, bal_b, resid_h, q1_h, k1_h, v1_h, q2_h, k2_h, v2_h, gain_a, gain_b, o1_h, o2_h,
    mlp_gain, up_h, down_h,
    out,
    resid, q1, k1, v1, q2, k2, v2, o1, o2, kv_own, q_own, kv_all, q_all, heads_out, heads_in,
    up_all, down_all, part, other_part, mixed, rows, hidden, terms, held, acc, relays, from_mate, from_across, result,
    fetch, kzs, kzr, qzs, qzr, kps, kpr, uzs, uzr, ups, upr, dzs, dzr, dps, dpr, hzs, hzr,
    sws, swr, rus, rds, rr, rcs, rcr, ts, tr, cus, cds, cbr, car, fs, fr,
):
    s = lax.axis_index("sp")
    c = lax.axis_index("tp")
    z = s // PLANE
    p = s % PLANE
    x = p % 2
    y = p // 2
    flip_x = y * 2 + 1 - x
    flip_y = (1 - y) * 2 + x
    near = (1 - c) * flip_x + c * flip_y
    side = (1 - c) * flip_y + c * flip_x
    far = (1 - y) * 2 + 1 - x
    to_near = (z * PLANE + near, c)
    to_side = (z * PLANE + side, c)
    to_core = (s, 1 - c)
    to_up = (s + PLANE, c)
    to_down = (s - PLANE, c)

    tokens = kv_own.shape[1]
    wide = gain_a.shape[1]
    deep = gain_b.shape[1]
    features = resid.shape[1]
    span = PLANE * tokens
    depth = up_h.shape[0]
    width = up_all.shape[1]
    half = tokens // 2
    unit = depth // 8
    sizes = {"up": (4 * unit, 4 * unit), "down": tuple(n * unit for n in (2, 2, 2, 2))}
    count_all = line * PLANE

    def begin(name, h):
        return sum(sizes[name][:h])

    def rows_of(name, h):
        return slice(begin(name, h), begin(name, h) + sizes[name][h])

    def columns_of(k):
        return slice(count_all * begin("down", k), count_all * begin("down", k + 1))

    def fetched(number, src, dst):
        return pltpu.make_async_copy(src, dst, fetch.at[number])

    def at_place(ref, number, size):
        return ref.at[pl.ds(pl.multiple_of(number * size, size), size)]

    def spot(name, h, number):
        size = sizes[name][h]
        if name == "up":
            return up_all.at[pl.ds(pl.multiple_of(number * depth + begin(name, h), unit), size)]
        return down_all.at[pl.ds(pl.multiple_of(count_all * begin(name, h) + number * size, unit), size)]

    small = [
        fetched(0, k1_h, k1), fetched(1, v1_h, v1), fetched(2, k2_h, k2), fetched(3, v2_h, v2),
        fetched(4, q1_h, q1), fetched(5, q2_h, q2),
    ]
    own_weights = {}
    for i, (name, source) in enumerate((("up", up_h), ("down", down_h))):
        for h in range(len(sizes[name])):
            block = source.at[rows_of(name, h), pl.ds(pl.multiple_of(z * width, width), width)]
            own_weights[name, h] = fetched(9 + 2 * i + h, block, spot(name, h, s))
    large = [fetched(6, resid_h, resid), fetched(7, o1_h, o1), fetched(8, o2_h, o2)]
    for copy in small + list(own_weights.values()) + large:
        copy.start()

    barrier = pltpu.get_barrier_semaphore()
    peers = [to_near, to_side, to_core] + [(((z + j) % line) * PLANE + p, c) for j in range(1, line)]
    for device in peers:
        pl.semaphore_signal(barrier, inc=1, device_id=device, device_id_type=MESH)

    sends = []

    def send(*args):
        copy = remote(*args)
        copy.start()
        sends.append((None, copy))

    def send_if(condition, *args):
        copy = remote(*args)

        @pl.when(condition)
        def _():
            copy.start()

        sends.append((condition, copy))

    def arrived(block, sem):
        remote(block, block, fs.at[0], sem, to_core).wait_recv()

    for copy in small:
        copy.wait()
    count = tokens * line
    order = lax.broadcasted_iota(jnp.int32, (count, count), 0)
    place = lax.broadcasted_iota(jnp.int32, (count, count), 1)
    pick = jnp.where(place == (order % tokens) * line + order // tokens, 1.0, 0.0).astype(jnp.bfloat16)

    def by_head(value):
        moved = jnp.dot(pick, value, preferred_element_type=jnp.float32).astype(jnp.bfloat16)
        return moved.reshape(line, tokens, value.shape[1])

    row = lax.broadcasted_iota(jnp.int32, (tokens, tokens), 0)
    column = lax.broadcasted_iota(jnp.int32, (tokens, tokens), 1)
    same = jnp.where(row == column, 1.0, 0.0).astype(jnp.bfloat16)
    kv_own[:, :, 0:wide] = by_head(k1[...])
    kv_own[:, :, wide:2 * wide] = by_head(v1[...])
    for h in range(line):
        turned = last(same, jnp.concatenate([k2[h], v2[h]], axis=0))
        kv_own[h, :, 2 * wide:3 * wide] = turned.astype(jnp.bfloat16)
    q_own[:, 0:tokens, :] = by_head(q1[...])
    for h in range(line):
        q_own[h, tokens:, :] = folded(last(same, q2[h]).astype(jnp.bfloat16))
    pl.semaphore_wait(barrier, len(peers))

    def ahead(j):
        number = z
        bit = 1
        while bit <= j:
            if j & bit:
                number = number + bit * (1 - 2 * ((number // bit) % 2))
            bit *= 2
        return number

    behind = ahead

    def z_peer(j):
        return (ahead(j) * PLANE + p, c)

    mine = at_place(kv_all, s, tokens)
    for j in range(1, line):
        send(kv_own.at[ahead(j)], mine, kzs.at[j], kzr.at[j], z_peer(j))
    send(kv_own.at[z], mine, kps.at[0, 0], kpr.at[0, 0], to_near)
    send(kv_own.at[z], mine, kps.at[0, 1], kpr.at[0, 1], to_side)
    mine[...] = kv_own[z]
    q_all[z] = q_own[z]

    def push(name, h, j):
        source = up_h if name == "up" else down_h
        block = source.at[rows_of(name, h), pl.ds(pl.multiple_of(ahead(j) * width, width), width)]
        ss, sr = (uzs, uzr) if name == "up" else (dzs, dzr)
        send(block, spot(name, h, s), ss.at[h, j], sr.at[h, j], z_peer(j))

    def plane_sems(name):
        return (ups, upr) if name == "up" else (dps, dpr)

    def spread(name, h, j):
        block = spot(name, h, behind(j) * PLANE + p)
        if j:
            arrived(block, (uzr if name == "up" else dzr).at[h, j])
        else:
            own_weights[name, h].wait()
        ss, sr = plane_sems(name)
        send(block, block, ss.at[h, j, 0], sr.at[h, j, 0], to_near)
        send(block, block, ss.at[h, j, 1], sr.at[h, j, 1], to_side)

    def relay(name, h, j):
        block = spot(name, h, behind(j) * PLANE + near)
        ss, sr = plane_sems(name)
        arrived(block, sr.at[h, j, 0])
        send(block, block, ss.at[h, j, 2], sr.at[h, j, 2], to_side)

    def settle(name, h, j):
        ss, sr = plane_sems(name)
        for way, where in ((1, side), (2, far)):
            arrived(spot(name, h, behind(j) * PLANE + where), sr.at[h, j, way])

    done = []
    lag = 2

    def flow(*items):
        for item in items:
            spread(*item)
            if len(done) >= lag:
                relay(*done[-lag])
            done.append(item)

    def drain():
        for item in done[-lag:]:
            relay(*item)

    def ask():
        for j in range(1, line):
            send(q_own.at[ahead(j)], q_all.at[z], qzs.at[j], qzr.at[j], z_peer(j))

    def kv_spread(j):
        block = at_place(kv_all, behind(j) * PLANE + p, tokens)
        arrived(block, kzr.at[j])
        send(block, block, kps.at[j, 0], kpr.at[j, 0], to_near)
        send(block, block, kps.at[j, 1], kpr.at[j, 1], to_side)

    def kv_relay(j):
        block = at_place(kv_all, behind(j) * PLANE + near, tokens)
        arrived(block, kpr.at[j, 0])
        send(block, block, kps.at[j, 2], kpr.at[j, 2], to_side)

    kv_spread(1)
    kv_relay(0)
    ask()
    kv_spread(2)
    kv_relay(1)
    push("up", 0, 1)
    kv_spread(3)
    push("down", 2, 3)
    push("up", 1, 1)
    kv_relay(2)
    kv_relay(3)
    push("down", 3, 3)
    for j in range(line):
        for way, where in ((1, side), (2, far)):
            arrived(at_place(kv_all, behind(j) * PLANE + where, tokens), kpr.at[j, way])
    for j in range(1, line):
        arrived(q_all.at[behind(j)], qzr.at[j])
    flow(("up", 0, 0))
    push("up", 0, 2)

    lanes_a = lax.broadcasted_iota(jnp.int32, (tokens, wide), 1)
    lanes_b = lax.broadcasted_iota(jnp.int32, (tokens, deep), 1)
    line_rows = lax.broadcasted_iota(jnp.int32, (2 * tokens, span), 0) % tokens + p * tokens
    visible = lax.broadcasted_iota(jnp.int32, (2 * tokens, span), 1) <= line_rows

    def mix(queries, lanes, keys_at, values_at, size, b, keys_number):
        zeros = jnp.zeros_like(queries)
        picked = jnp.concatenate(
            [jnp.where(lanes < size, queries, zeros), jnp.where(lanes < size, zeros, queries)], axis=0
        )
        scores = last(picked, kv_all[0:keys_number, keys_at])
        tail_scores = jnp.where(visible, scores[:, keys_number - span:], -jnp.inf)
        if keys_number > span:
            scores = jnp.concatenate([scores[:, : keys_number - span], tail_scores], axis=1)
        else:
            scores = tail_scores
        gaps = scores - jnp.max(scores, axis=-1, keepdims=True)
        powers = jnp.exp2(gaps * (size ** (-0.5) * math.log2(math.e)))
        sums = jnp.sum(powers, axis=-1, keepdims=True)
        mixing = powers[:tokens] * (1.0 / sums[:tokens]) - powers[tokens:] * (b / sums[tokens:])
        return jnp.dot(
            mixing.astype(jnp.bfloat16), kv_all[0:keys_number, values_at], preferred_element_type=jnp.float32
        )

    def norm(value, gain):
        power = jnp.mean(value * value, axis=-1, keepdims=True)
        return (value * lax.rsqrt(power + EPSILON) * gain[...] * HEAD_SCALE).astype(jnp.bfloat16)

    def tile(j):
        number = (j + 1) * span
        first = mix(
            q_all[j, 0:tokens, :], lanes_a, slice(0, wide), slice(wide, 2 * wide), size_a, bal_a[z], number
        )
        heads_out[j, 0:tokens, :] = norm(first, gain_a)
        second = mix(
            unfolded(q_all[j, tokens:, :]), lanes_b, slice(2 * wide, 2 * wide + deep),
            slice(2 * wide, 3 * wide), size_b, bal_b[z], number,
        )
        heads_out[j, tokens:, :] = folded(norm(second[:, wide - deep:wide], gain_b))
        send_if(j != z, heads_out.at[j], heads_in.at[z], hzs.at[j], hzr.at[z], (j * PLANE + p, c))

    tile(3)

    tile(2)
    flow(("up", 1, 0))
    push("up", 1, 2)
    tile(1)

    tile(0)
    heads_in[z] = heads_out[z]
    push("up", 0, 3)
    push("down", 0, 1)
    push("down", 1, 1)
    flow(("down", 0, 0))
    flow(("down", 1, 0))
    flow(("down", 2, 0))
    push("up", 1, 3)
    flow(("up", 0, 1))
    flow(("down", 3, 0))
    flow(("up", 1, 1))
    for copy in large:
        copy.wait()
    for h in range(line):
        block = heads_in.at[h]

        @pl.when(h != z)
        def _():
            arrived(block, hzr.at[h])

    heads_first = jnp.concatenate([heads_in[h, 0:tokens, :] for h in range(line)], axis=1)
    heads_second = jnp.concatenate([unfolded(heads_in[h, tokens:, :]) for h in range(line)], axis=1)
    step = features // 4
    for n in range(4):
        at = slice(n * step, (n + 1) * step)
        value = jnp.dot(heads_first, o1[:, at], preferred_element_type=jnp.float32) + jnp.dot(
            heads_second, o2[:, at], preferred_element_type=jnp.float32
        )
        part[:, :, at] = value.astype(jnp.bfloat16).reshape(2, half, step)
    swap = remote(part.at[1 - c], other_part, sws.at[0], swr.at[0], to_core)
    swap.start()
    flow(("up", 0, 2))
    swap.wait()
    both = part[c].astype(jnp.float32) + other_part[...].astype(jnp.float32)
    mine_rows = pl.ds(pl.multiple_of(c * half, half), half)
    mixed[...] = (resid[mine_rows, :].astype(jnp.float32) + both).astype(jnp.bfloat16)
    whole = mixed[...].astype(jnp.float32)
    power = jnp.mean(whole * whole, axis=-1, keepdims=True)
    own_slot = at_place(rows, z * 2 + c, half)
    own_slot[...] = (whole * lax.rsqrt(power + EPSILON) * mlp_gain[...]).astype(jnp.bfloat16)

    send_if(z < line - 1, own_slot, own_slot, rus.at[0], rr.at[z], to_up)
    send_if(z > 0, own_slot, own_slot, rds.at[0], rr.at[z], to_down)
    send(own_slot, own_slot, rcs.at[0], rcr.at[z], to_core)

    def rows_low(d):
        low = jnp.maximum(z - d, 0)
        from_low = at_place(rows, low * 2 + c, half)

        @pl.when(z >= d)
        def _():
            arrived(from_low, rr.at[low])

        send_if((z >= d) & (z < line - 1), from_low, from_low, rus.at[d], rr.at[low], to_up)
        send_if(z >= d, from_low, from_low, rcs.at[d], rcr.at[low], to_core)

    def rows_high(d):
        high = jnp.minimum(z + d, line - 1)
        from_high = at_place(rows, high * 2 + c, half)

        @pl.when(z + d < line)
        def _():
            arrived(from_high, rr.at[high])

        send_if((z + d < line) & (z > 0), from_high, from_high, rds.at[d], rr.at[high], to_down)
        send_if(z + d < line, from_high, from_high, rcs.at[line - 1 + d], rcr.at[high], to_core)

    flow(("up", 1, 2))
    flow(("up", 0, 3))
    push("down", 0, 2)
    push("down", 1, 2)
    rows_low(1)
    rows_high(1)
    push("down", 0, 3)
    push("down", 1, 3)
    push("down", 2, 1)
    flow(("up", 1, 3))
    flow(("down", 0, 1))
    flow(("down", 1, 1))
    push("down", 3, 1)
    rows_low(2)
    rows_high(2)
    flow(("down", 1, 2))
    push("down", 2, 2)
    push("down", 3, 2)
    flow(("down", 0, 2))
    flow(("down", 0, 3))
    flow(("down", 1, 3))
    rows_low(3)
    rows_high(3)
    flow(("down", 2, 1))
    flow(("down", 3, 1))
    lift = 256

    def raise_rows():
        for k in range(line):
            arrived(at_place(rows, k * 2 + 1 - c, half), rcr.at[k])
        for h in range(2):
            for j in range(line):
                settle("up", h, j)

        @pl.loop(0, width // lift)
        def _(n):
            at = pl.ds(pl.multiple_of(n * lift, lift), lift)
            lifted = jnp.maximum(jnp.dot(rows[...], up_all[:, at], preferred_element_type=jnp.float32), 0.0)
            hidden[:, at] = (lifted * lifted).astype(jnp.bfloat16)

    def chunk(k):
        at = columns_of(k)
        value = last(hidden[...], down_all[at, :]).astype(jnp.bfloat16)
        terms[:, :, :, at] = value.reshape(line, 2, half, at.stop - at.start)
        send(terms.at[:, 1 - c, :, at], held.at[:, :, at], ts.at[k], tr.at[k], to_core)

    upper = z // 2
    ends = (z == 0) | (z == line - 1)
    inner = (z > 0) & (z < line - 1)
    mate = ahead(1)
    to_mate = (mate * PLANE + p, c)
    across = [2 - upper, (1 - upper) * (line - 1)]

    def combine(k):
        at = columns_of(k)
        arrived(held.at[:, :, at], tr.at[k])
        for zd in range(line):
            acc[zd, :, at] = add(terms[zd, c, :, at], held[zd, :, at])
        for r in (1, 0):
            block = acc.at[across[r], :, at]
            send_if(ends, block, relays.at[r, :, at], cus.at[r, k], cbr.at[r, k], to_mate)
        send(acc.at[mate, :, at], from_mate.at[:, at], cds.at[0, k], car.at[0, k], to_mate)

    def cross(k):
        at = columns_of(k)
        for r in (1, 0):
            block = acc.at[across[r], :, at]

            @pl.when(inner)
            def _():
                arrived(relays.at[r, :, at], cbr.at[r, k])
                block[...] = add(block[...], relays[r, :, at])

            send_if(
                inner, block, from_across.at[:, at], cus.at[2 + r, k], car.at[1, k],
                (across[r] * PLANE + p, c),
            )

    def finish(k):
        at = columns_of(k)
        arrived(from_mate.at[:, at], car.at[0, k])
        arrived(from_across.at[:, at], car.at[1, k])
        value = acc[z, :, at].astype(jnp.float32) + from_mate[:, at].astype(jnp.float32)
        value = value + from_across[:, at].astype(jnp.float32)
        size = sizes["down"][k]
        for i in range(count_all):
            to = slice(i * depth + begin("down", k), i * depth + begin("down", k + 1))
            term = value[:, i * size:(i + 1) * size]
            result[:, to] = (mixed[:, to].astype(jnp.float32) + term).astype(jnp.bfloat16)
        if k == line - 1:
            send(result, out.at[c], fs.at[0], fr.at[0], to_core)
            fetched(10 + line, result, out.at[c]).start()

    raise_rows()
    flow(("down", 2, 2))
    for j in range(line):
        settle("down", 0, j)
    chunk(0)
    for j in range(line):
        settle("down", 1, j)
    chunk(1)
    flow(("down", 2, 3))
    combine(0)
    combine(1)
    flow(("down", 3, 2))
    flow(("down", 3, 3))
    drain()
    cross(0)
    for j in range(line):
        settle("down", 2, j)
    chunk(2)
    combine(2)
    cross(1)
    for j in range(line):
        settle("down", 3, j)
    chunk(3)
    combine(3)
    finish(0)
    cross(2)
    finish(1)
    cross(3)
    finish(2)
    finish(3)
    arrived(out.at[1 - c], fr.at[0])
    fetched(10 + line, result, out.at[c]).wait()
    for condition, copy in sends:
        if condition is None:
            copy.wait_send()
        else:

            @pl.when(condition)
            def _():
                copy.wait_send()


def layer(
    line, residual, q1, k1, v1, q2, k2, v2, bal_a, bal_b, gain_a, gain_b, o1, o2, mlp_gain, up, down
):
    tokens, features = residual.shape
    half = tokens // 2
    wide = v1.shape[1]
    n = line * PLANE
    width = up.shape[1] // line
    depth = up.shape[0]
    b16 = jnp.bfloat16
    dma = pltpu.SemaphoreType.DMA
    vmem = pl.BlockSpec(memory_space=pltpu.VMEM)
    smem = pl.BlockSpec(memory_space=pltpu.SMEM)
    any_ = pl.BlockSpec(memory_space=pl.ANY)

    def buffer(*shape):
        return pltpu.VMEM(shape, b16)

    return pl.pallas_call(
        functools.partial(layer_kernel, line, q1.shape[1] // 2, q2.shape[1] // 2),
        out_shape=jax.ShapeDtypeStruct((2, half, features), b16),
        in_specs=[smem, smem] + [any_] * 7 + [vmem, vmem, any_, any_, vmem, any_, any_],
        out_specs=any_,
        scratch_shapes=[
            buffer(tokens, features), buffer(*q1.shape), buffer(*k1.shape), buffer(*v1.shape),
            buffer(*q2.shape), buffer(*k2.shape), buffer(*v2.shape), buffer(*o1.shape), buffer(*o2.shape),
            buffer(line, tokens, 3 * wide), buffer(line, tokens + half, wide),
            buffer(n * tokens, 3 * wide), buffer(line, tokens + half, wide),
            buffer(line, tokens + half, wide), buffer(line, tokens + half, wide),
            buffer(n * depth, width), buffer(n * depth, width),
            buffer(2, half, features), buffer(half, features), buffer(half, features),
            buffer(line * tokens, features), buffer(line * tokens, width),
            buffer(line, 2, half, features), buffer(line, half, features), buffer(line, half, features),
            buffer(2, half, features), buffer(half, features), buffer(half, features), buffer(half, features),
            dma((11 + line,)),
            dma((line,)), dma((line,)), dma((line,)), dma((line,)), dma((line, 3)), dma((line, 3)),
            dma((2, line)), dma((2, line)), dma((2, line, 3)), dma((2, line, 3)),
            dma((line, line)), dma((line, line)), dma((line, line, 3)), dma((line, line, 3)),
            dma((line,)), dma((line,)), dma((1,)), dma((1,)),
            dma((line,)), dma((line,)), dma((line,)), dma((2 * line - 1,)), dma((line,)),
            dma((line,)), dma((line,)), dma((line, line)), dma((1, line)),
            dma((2, line)), dma((2, line)), dma((1,)), dma((1,)),
        ],
        compiler_params=pltpu.CompilerParams(
            collective_id=0, has_side_effects=True, vmem_limit_bytes=60 * 1024 * 1024
        ),
    )(bal_a, bal_b, residual, q1, k1, v1, q2, k2, v2, gain_a, gain_b, o1, o2, mlp_gain, up, down)


def placed_body(
    residual, query_first, key_first, value_first, query_second, key_second, value_second,
    balance_first, balance_second, head_gain_first, head_gain_second, out_first, out_second,
    mlp_gain, up_weight, down_weight,
):
    tokens, line, _ = query_first.shape

    def flat(array):
        return array.reshape(tokens * line, array.shape[2])

    def turned(array):
        return array.transpose(1, 2, 0)

    out = layer(
        line, residual, flat(query_first), flat(key_first), flat(value_first), turned(query_second),
        turned(key_second), turned(value_second), balance_first, balance_second,
        head_gain_first[None, :], head_gain_second[None, :], out_first, out_second,
        mlp_gain[None, :], up_weight, down_weight,
    )
    return out.reshape(residual.shape)


def placed(mesh):
    ranks = mesh.shape["sp"]
    cores = mesh.shape["tp"]
    return cores == 2 and ranks % PLANE == 0


def choose(mesh):
    ranks = mesh.shape["sp"]

    def run(*arrays):
        query_first, query_second, value_second, value_first = arrays[1], arrays[4], arrays[6], arrays[3]
        fits = (
            placed(mesh)
            and ranks == PLANE * PLANE
            and arrays[14].shape[0] % 128 == 0
            and query_first.shape[1] * PLANE == ranks
            and query_second.shape[1] == query_first.shape[1]
            and value_first.shape[2] == query_first.shape[2] == 128
            and query_second.shape[2] * 2 == value_second.shape[2] * 2 == query_first.shape[2]
            and query_first.shape[0] % 32 == 0
            and arrays[14].shape[1] % (128 * ranks) == 0
        )
        return (placed_body if fits else body)(*arrays)

    return run


def solution(mesh):
    in_specs = (
        P("sp", None),
        P("sp", "tp", None),
        P("sp", "tp", None),
        P("sp", "tp", None),
        P("sp", "tp", None),
        P("sp", "tp", None),
        P("sp", "tp", None),
        P("tp"),
        P("tp"),
        P(),
        P(),
        P("tp", None),
        P("tp", None),
        P(),
        P("sp", "tp"),
        P("sp", "tp"),
    )
    out_specs = P("sp", None)
    return jax.shard_map(choose(mesh), mesh=mesh, in_specs=in_specs, out_specs=out_specs, check_vma=False)
```
